32 devices in a mesh: ep: 8 (over z, y), tp: 4 (over x, core).
Axes of the slice: x: 2, y: 2, z: 4, core: 2. Of those that a mesh axis runs over, the one named last changes fastest.
Arguments:
- hidden: bfloat16 [512, 2048], P('ep'), may hold values from -10 to 10
- mix_gain: bfloat16 [2048], replicated, may hold values from 0.099609375 to 1.8984375
- proj_x: bfloat16 [2048, 2048], P('ep', 'tp'), may hold values from -0.125 to 0.125
- proj_y: bfloat16 [2048, 2048], P('ep', 'tp'), may hold values from -0.125 to 0.125
- conv_taps: bfloat16 [4, 2048], P(None, 'tp'), may hold values from -3 to 3
- input_gate: bfloat16 [32, 64, 64], P('tp'), may hold values from -0.75 to 0.75
- decay_gate: bfloat16 [32, 64, 64], P('tp'), may hold values from -0.75 to 0.75
- decay_param: float32 [2048], P('tp'), may hold values from 1 to 6
- proj_out: bfloat16 [2048, 2048], P('tp'), may hold values from -0.125 to 0.125
- conv_state: bfloat16 [512, 3, 2048], P('ep', None, 'tp'), may hold values from -6 to 6
- lru_state: float32 [512, 2048], P('ep', 'tp'), may hold values from -6 to 6
- ffn_gain: bfloat16 [2048], replicated, may hold values from 0.099609375 to 1.8984375
- routes: int32 [512, 2], P('ep'), may hold values from 0 to 7, all different within a row; in each aligned block of 64 rows (0 to 63, 64 to 127, ...) at most 18 rows name the same one
- route_weights: float32 [512, 2], P('ep'), may hold values from 0.2 to 1
- expert_gate: bfloat16 [8, 2048, 3072], P('ep', None, 'tp'), may hold values from -0.125 to 0.125
- expert_up: bfloat16 [8, 2048, 3072], P('ep', None, 'tp'), may hold values from -0.125 to 0.125
- expert_down: bfloat16 [8, 3072, 2048], P('ep', 'tp'), may hold values from -0.109375 to 0.109375
- dense_gate: bfloat16 [2048, 6144], P('tp', 'ep'), may hold values from -0.125 to 0.125
- dense_up: bfloat16 [2048, 6144], P('tp', 'ep'), may hold values from -0.125 to 0.125
- dense_down: bfloat16 [6144, 2048], P('ep', 'tp'), may hold values from -0.078125 to 0.078125
- branch_gate: float32 [2048], P('tp'), may hold values from -4 to 4
Outputs:
- new_hidden: bfloat16 [512, 2048], P('ep', 'tp')
- new_lru: float32 [512, 2048], P('ep', 'tp')
- new_conv: bfloat16 [512, 3, 2048], P('ep', None, 'tp')
The draws below stay inside these ranges and needn't reach their ends.
Inputs may be any that keep to these rules, and one draw needn't show every extreme that they name: `routes`: each row names 2 different experts. In the 64 rows of one index of ep, no expert is named by more than 18 rows, a bound that some block reaches.
All inputs are finite; a program needn't handle non-finite values.
Results may differ from the reference program's by a relative error of at most 0.017.
Values may be sent and summed in bfloat16 or wider, within the bound.
No kernel may reach another device: no remote copies, remote signals or barrier semaphores. Data moves between devices by JAX's collectives and lax.ppermute only.
A program may use at most 128 MiB of HBM per device.

```python
import math
import jax
import jax.numpy as jnp
import numpy as np
from jax import lax

D = 2048
HEADS = 32
BLOCK = 64
LRU = 2048
TAPS = 4
FFE = 3072
DFF = 6144
EXPERTS = 8
TOPK = 2
SEQ_DEV = 64
BATCH = 512
CAP = 18
N_EP = 8
N_TP = 4


def draw_hidden(key, part):
    noise_key = jax.random.fold_in(key, 11)
    column = jnp.arange(D, dtype=jnp.float32) / (D - 1)
    scales = 0.5 * jnp.power(4.0, column)
    values = jax.random.normal(noise_key, (BATCH, D), jnp.float32) * scales[None, :]
    return jnp.clip(values, -10.0, 10.0).astype(jnp.bfloat16)


def shard_levels(rng, shape, cuts, smallest, top_value):
    loudness = 1.0
    for dim, shards_of in cuts:
        draws = jax.random.uniform(jax.random.fold_in(jax.random.fold_in(rng, 6), dim), (shards_of,), jnp.float32, smallest / len(cuts), top_value / len(cuts))
        loudness = loudness * jnp.repeat(jnp.exp(draws), shape[dim] // shards_of).reshape((-1,) + (1,) * (len(shape) - 1 - dim))
    return loudness


def assign_block(key, own, number, rows, count, top, reach, slope):
    sequence = jax.random.permutation(key, count)
    crowded, common = portions_of(count, rows * top, reach, slope, True), portions_of(count, rows * top, reach, slope, False)
    places = jnp.arange(count)

    def named(lengths, turn):
        used = int((lengths > 0).sum())
        fixed = max(1, used // 4)
        passed = fixed + (places - fixed + turn * (used - fixed)) % max(1, count - fixed)
        return jnp.zeros((count,), jnp.int32).at[sequence[jnp.where(places < fixed, places, passed)]].set(jnp.asarray(lengths, jnp.int32))

    lengths = jnp.where(number % 4 == 0, named(crowded, number // 4), named(common, number - number // 4 - 1))
    mixed = jax.random.permutation(jax.random.fold_in(own, 3), count)
    source_of, receiver = mixed[0:count // 2 * 2:2], mixed[1:count // 2 * 2:2]
    margin = jnp.minimum(lengths[source_of] - 1, reach - lengths[receiver]) // 2
    margin = jnp.where((source_of == sequence[0]) | (receiver == sequence[0]) | (lengths[receiver] == 0), 0, jnp.maximum(margin, 0))
    passed = jax.random.randint(jax.random.fold_in(own, 4), (count // 2,), 0, 1 << 20) % (margin + 1)
    lengths = lengths.at[source_of].add(-passed).at[receiver].add(passed)
    labels = jnp.searchsorted(jnp.cumsum(lengths), jnp.arange(rows * top), side="right").astype(jnp.int32)
    listing = labels.reshape(top, rows).T
    listing = listing[jax.random.permutation(jax.random.fold_in(own, 1), rows)]
    turn = jax.random.randint(jax.random.fold_in(own, 2), (rows, 1), 0, top)
    return jnp.take_along_axis(listing, (jnp.arange(top)[None, :] + turn) % top, axis=1)


def portions_of(count, total, limit, lean, full):
    portions = [(1 << 20) // math.isqrt(rank ** lean) + 1 for rank in range(1, count + 1)]
    largest = limit if full else min(limit, max(-(-total // count), total * portions[0] // sum(portions)))
    least = 1 if total - largest >= count - 1 else 0
    counts, rest = [largest] + [least] * (count - 1), total - largest - least * (count - 1)
    while rest > 0:
        movable = [i for i in range(1, count) if counts[i] < largest] or [i for i in range(1, count) if counts[i] < limit]
        whole, budget = sum([portions[i] for i in movable]), rest
        for i in movable:
            addition = min(limit - counts[i], max(1, budget * portions[i] // whole), rest)
            counts[i] = counts[i] + addition
            rest = rest - addition
    return np.array(counts)


def bell_draw(stream_key, dims, spread, reach, split=(), held_as=jnp.bfloat16):
    values = jax.random.normal(stream_key, dims, jnp.float32) * spread
    if len(split) > 0:
        values = shard_levels(stream_key, dims, split, -0.22, 0.18) * values
    return jnp.clip(values, min=-reach, max=reach).astype(held_as)


def setup_inputs(seed: int = 0) -> dict:
    streams_of = jax.random.split(jax.random.key(seed), 22)
    hidden = draw_hidden(jax.random.fold_in(streams_of[21], 71), 0)
    mix_gain = jnp.clip(1.0 + 0.18 * jax.random.normal(streams_of[1], (D,), jnp.float32), 0.099609375, 1.8984375).astype(jnp.bfloat16)
    proj_x = bell_draw(streams_of[2], (D, LRU), D ** -0.5, 0.125, ((0, 8), (1, 4)))
    proj_y = bell_draw(streams_of[3], (D, LRU), D ** -0.5, 0.125, ((0, 8), (1, 4)))
    conv_taps = bell_draw(streams_of[4], (TAPS, LRU), 0.5, 3.0, ((1, 4),))
    input_gate = bell_draw(streams_of[5], (HEADS, BLOCK, BLOCK), BLOCK ** -0.5, 0.75, ((0, 4),))
    decay_gate = bell_draw(streams_of[6], (HEADS, BLOCK, BLOCK), BLOCK ** -0.5, 0.75, ((0, 4),))
    decay_param = jnp.clip(1.0 + 5.0 * jax.random.uniform(streams_of[7], (LRU,), jnp.float32) ** shard_levels(streams_of[7], (LRU,), ((0, 4),), -0.2, 0.2), 1.0, 6.0)
    proj_out = bell_draw(streams_of[8], (LRU, D), LRU ** -0.5, 0.125, ((0, 4),))
    conv_state = bell_draw(streams_of[9], (BATCH, TAPS - 1, LRU), 1.0, 6.0, ((0, 8), (2, 4)))
    lru_state = bell_draw(streams_of[10], (BATCH, LRU), 1.0, 6.0, ((0, 8), (1, 4)), jnp.float32)
    ffn_gain = jnp.clip(1.0 + 0.18 * jax.random.normal(streams_of[11], (D,), jnp.float32), 0.099609375, 1.8984375).astype(jnp.bfloat16)
    routes_keys = jax.random.split(jax.random.fold_in(streams_of[12], 1), BATCH // SEQ_DEV)
    routes_turns = jax.random.permutation(jax.random.fold_in(streams_of[12], 3), BATCH // SEQ_DEV)
    routes = jax.vmap(lambda own, number: assign_block(jax.random.fold_in(streams_of[12], 2), own, number, SEQ_DEV, EXPERTS, TOPK, CAP, 1))(routes_keys, routes_turns).reshape((BATCH, TOPK))
    route_weights = jnp.clip(jnp.exp(math.log(1.0) - 1.609438 * jax.random.uniform(streams_of[13], (BATCH, TOPK), jnp.float32) ** shard_levels(streams_of[13], (BATCH, TOPK), ((0, 8),), -0.2, 0.2)), 0.2, 1.0)
    expert_gate = bell_draw(streams_of[14], (EXPERTS, D, FFE), D ** -0.5, 0.125, ((0, 8), (2, 4)))
    expert_up = bell_draw(streams_of[15], (EXPERTS, D, FFE), D ** -0.5, 0.125, ((0, 8), (2, 4)))
    expert_down = bell_draw(streams_of[16], (EXPERTS, FFE, D), FFE ** -0.5, 0.109375, ((0, 8), (1, 4)))
    dense_gate = bell_draw(streams_of[17], (D, DFF), D ** -0.5, 0.125, ((0, 4), (1, 8)))
    dense_up = bell_draw(streams_of[18], (D, DFF), D ** -0.5, 0.125, ((0, 4), (1, 8)))
    dense_down = bell_draw(streams_of[19], (DFF, D), DFF ** -0.5, 0.078125, ((0, 8), (1, 4)))
    branch_gate = bell_draw(streams_of[20], (D,), 1.0, 4.0, ((0, 4),), jnp.float32)
    return dict(hidden=hidden, mix_gain=mix_gain, proj_x=proj_x, proj_y=proj_y, conv_taps=conv_taps, input_gate=input_gate, decay_gate=decay_gate, decay_param=decay_param, proj_out=proj_out, conv_state=conv_state, lru_state=lru_state, ffn_gain=ffn_gain, routes=routes, route_weights=route_weights, expert_gate=expert_gate, expert_up=expert_up, expert_down=expert_down, dense_gate=dense_gate, dense_up=dense_up, dense_down=dense_down, branch_gate=branch_gate)


epsilon = 1e-06
decay_scale = 8.0

def rms_scale(values, gain_vec):
    floats = values.astype(jnp.float32)
    meansq = lax.optimization_barrier(jnp.mean(floats * floats, axis=-1, keepdims=True))
    return floats * lax.rsqrt(meansq + epsilon) * gain_vec.astype(jnp.float32)

def reference(hidden, mix_gain, proj_x, proj_y, conv_taps, input_gate, decay_gate, decay_param, proj_out, conv_state, lru_state, ffn_gain, routes, route_weights, expert_gate, expert_up, expert_down, dense_gate, dense_up, dense_down, branch_gate):
    batch_rows = hidden.shape[0]
    lru_width = HEADS * BLOCK
    normed = rms_scale(hidden, mix_gain).astype(jnp.bfloat16)
    x_proj = jnp.dot(normed, proj_x, preferred_element_type=jnp.float32).astype(jnp.bfloat16)
    y_proj = jnp.dot(normed, proj_y, preferred_element_type=jnp.float32).astype(jnp.bfloat16)
    window = jnp.concatenate([conv_state, x_proj[:, None, :]], axis=1)
    conv_out = lax.optimization_barrier(jnp.sum(window.astype(jnp.float32) * conv_taps.astype(jnp.float32)[None], axis=1)).astype(jnp.bfloat16)
    heads_in = conv_out.astype(jnp.float32).reshape(batch_rows, HEADS, BLOCK)
    gate_in = jax.nn.sigmoid(jnp.einsum('bhi,hij->bhj', heads_in, input_gate.astype(jnp.float32)).reshape(batch_rows, lru_width))
    gate_dec = jax.nn.sigmoid(jnp.einsum('bhi,hij->bhj', heads_in, decay_gate.astype(jnp.float32)).reshape(batch_rows, lru_width))
    log_decay = decay_scale * gate_dec * jax.nn.log_sigmoid(decay_param)
    decay_rate = jnp.exp(log_decay)
    inject = jnp.sqrt(-jnp.expm1(2.0 * log_decay))
    new_lru = decay_rate * lru_state + inject * gate_in * conv_out.astype(jnp.float32)
    gated_out = (new_lru * jax.nn.gelu(y_proj.astype(jnp.float32))).astype(jnp.bfloat16)
    head_share = lru_width // N_TP
    mixer_sum = jnp.zeros((batch_rows, D), jnp.float32)
    for member in range(N_TP):
        partial_value = jnp.dot(gated_out[:, member * head_share:(member + 1) * head_share], proj_out[member * head_share:(member + 1) * head_share], preferred_element_type=jnp.float32).astype(jnp.bfloat16)
        mixer_sum = mixer_sum + partial_value.astype(jnp.float32)
    summed = (hidden.astype(jnp.float32) + mixer_sum).astype(jnp.bfloat16)
    ffn_in = rms_scale(summed, ffn_gain).astype(jnp.bfloat16)
    pair_expert = routes.reshape(-1).astype(jnp.int32)
    onehot = (pair_expert[:, None] == jnp.arange(EXPERTS, dtype=jnp.int32)[None, :]).astype(jnp.int32)
    grouped = onehot.reshape(N_EP, SEQ_DEV * TOPK, EXPERTS)
    before = jnp.cumsum(grouped, axis=1) - grouped
    slot_rank = lax.optimization_barrier(jnp.sum(before * grouped, axis=2)).reshape(-1)
    group_of = jnp.arange(BATCH * TOPK, dtype=jnp.int32) // (SEQ_DEV * TOPK)
    position = (group_of * CAP + slot_rank).astype(jnp.int32)
    token_of = jnp.arange(BATCH * TOPK, dtype=jnp.int32) // TOPK
    buffer = jnp.zeros((EXPERTS, N_EP * CAP, D), jnp.bfloat16).at[pair_expert, position].set(ffn_in[token_of])
    ff_share = FFE // N_TP

    def one_expert(operands):
        slot_rows, gate_w, up_w, down_w = operands
        gate_val = jnp.dot(slot_rows, gate_w, preferred_element_type=jnp.float32)
        up_val = jnp.dot(slot_rows, up_w, preferred_element_type=jnp.float32)
        inner_act = (jax.nn.silu(gate_val) * up_val).astype(jnp.bfloat16)
        total_out = jnp.zeros((slot_rows.shape[0], D), jnp.float32)
        for member in range(N_TP):
            piece_out = jnp.dot(inner_act[:, member * ff_share:(member + 1) * ff_share], down_w[member * ff_share:(member + 1) * ff_share], preferred_element_type=jnp.float32).astype(jnp.bfloat16)
            total_out = total_out + piece_out.astype(jnp.float32)
        return total_out.astype(jnp.bfloat16)
    results = lax.map(one_expert, (buffer, expert_gate, expert_up, expert_down))
    picked = results[pair_expert, position].astype(jnp.float32)
    expert_sum = lax.optimization_barrier(jnp.sum((picked * route_weights.reshape(-1)[:, None]).reshape(batch_rows, TOPK, D), axis=1))
    dense_g = jnp.dot(ffn_in, dense_gate, preferred_element_type=jnp.float32)
    dense_u = jnp.dot(ffn_in, dense_up, preferred_element_type=jnp.float32)
    dense_hid = (jax.nn.silu(dense_g) * dense_u).astype(jnp.bfloat16)
    dense_out = jnp.dot(dense_hid, dense_down, preferred_element_type=jnp.float32)
    new_hidden = (summed.astype(jnp.float32) + expert_sum + jax.nn.sigmoid(branch_gate)[None, :] * dense_out).astype(jnp.bfloat16)
    return (new_hidden, new_lru, window[:, 1:])
```

```python
import jax
import jax.numpy as jnp
from jax import lax
from jax.sharding import PartitionSpec as P

epsilon = 1e-06
decay_scale = 8.0
bf16 = jnp.bfloat16
f32 = jnp.float32


def row_rsqrt(floats):
    return lax.rsqrt(jnp.mean(floats * floats, axis=-1, keepdims=True) + epsilon)


def swap(value, axis, bits):
    size = lax.axis_size(axis)
    return lax.ppermute(value, axis, [(i, i ^ bits) for i in range(size)])


def dot(a, b):
    return jnp.dot(a, b, preferred_element_type=f32)


def spread_two_stage(value, axis):
    size = lax.axis_size(axis)
    blocks = {0: value}
    bit = size // 2
    while bit:
        blocks.update({k ^ bit: swap(b, axis, bit) for k, b in list(blocks.items())})
        bit //= 2
    return [blocks[k] for k in range(size)]


def spread_direct(value, axis):
    return [value] + [swap(value, axis, k) for k in range(1, lax.axis_size(axis))]


def on_device(
    hidden,
    mix_gain,
    proj_x,
    proj_y,
    conv_taps,
    input_gate,
    decay_gate,
    decay_param,
    proj_out,
    conv_state,
    lru_state,
    ffn_gain,
    routes,
    route_weights,
    expert_gate,
    expert_up,
    expert_down,
    dense_gate,
    dense_up,
    dense_down,
    branch_gate,
):
    tok_rows, width = hidden.shape
    ep_size = lax.axis_size("ep")
    tp_size = lax.axis_size("tp")
    ep_at = lax.axis_index("ep")
    tp_at = lax.axis_index("tp")
    col_width = width // tp_size
    lru_local = lru_state.shape[1]
    far = ep_size // 2
    near = ep_at % 2
    far_at = ep_at // 2

    other_x = swap(proj_x, "ep", 1)
    other_y = swap(proj_y, "ep", 1)
    dense_rows = spread_two_stage(jnp.concatenate([dense_gate, dense_up], axis=1), "tp")

    floats = hidden.astype(f32)
    normed = (floats * row_rsqrt(floats) * mix_gain.astype(f32)).astype(bf16)
    far_width = width // far
    spread = []
    for k in range(far):
        cols = lax.dynamic_slice_in_dim(normed, (far_at ^ k) * far_width, far_width, 1)
        spread.append(swap(cols, "ep", 2 * k) if k else cols)
    spread = jnp.concatenate(spread, axis=0)

    def both_rows(own, other):
        upper = jnp.where(near == 0, own, other)
        lower = jnp.where(near == 0, other, own)
        return jnp.concatenate([upper, lower], axis=0)

    part_x = dot(spread, both_rows(proj_x, other_x))
    part_y = dot(spread, both_rows(proj_y, other_y))
    parts = jnp.concatenate([part_x, part_y], axis=1).astype(bf16)
    parts = parts.reshape(far, tok_rows, 2 * lru_local)
    projected = parts[0].astype(f32)
    for k in range(1, far):
        projected = projected + swap(parts[k], "ep", 2 * k).astype(f32)
    x_proj = projected[:, :lru_local].astype(bf16)
    y_proj = projected[:, lru_local:].astype(bf16)

    window = jnp.concatenate([conv_state, x_proj[:, None, :]], axis=1)
    conv_out = jnp.sum(window.astype(f32) * conv_taps.astype(f32)[None], axis=1).astype(bf16)
    heads_here = input_gate.shape[0]
    block_size = input_gate.shape[1]
    heads_in = conv_out.reshape(tok_rows, heads_here, block_size)
    gate_in = jax.nn.sigmoid(
        jnp.einsum("bhi,hij->bhj", heads_in, input_gate, preferred_element_type=f32).reshape(
            tok_rows, lru_local
        )
    )
    gate_dec = jax.nn.sigmoid(
        jnp.einsum("bhi,hij->bhj", heads_in, decay_gate, preferred_element_type=f32).reshape(
            tok_rows, lru_local
        )
    )
    log_decay = decay_scale * gate_dec * jax.nn.log_sigmoid(decay_param)
    decay_rate = jnp.exp(log_decay)
    inject = jnp.sqrt(-jnp.expm1(2.0 * log_decay))
    new_lru = decay_rate * lru_state + inject * gate_in * conv_out.astype(f32)
    gated_out = (new_lru * jax.nn.gelu(y_proj.astype(f32))).astype(bf16)

    top_count = routes.shape[1]
    local_experts = expert_gate.shape[0]
    experts_all = local_experts * ep_size
    capacity = tok_rows * top_count // experts_all + 2
    padded = -(-(capacity + 1) // 8) * 8
    expert_ids = (ep_at ^ jnp.arange(ep_size, dtype=jnp.int32))[:, None] * local_experts
    expert_ids = (expert_ids + jnp.arange(local_experts, dtype=jnp.int32)[None, :]).reshape(-1)
    named = routes.T[None] == expert_ids[:, None, None]
    hit = jnp.any(named, axis=1)
    weight_hit = jnp.sum(jnp.where(named, route_weights.T[None], 0.0), axis=1)
    order = jnp.arange(tok_rows, dtype=jnp.int32)
    rank = dot(hit.astype(bf16), (order[:, None] < order[None, :]).astype(bf16))
    rank = jnp.where(hit, rank, -1.0).astype(jnp.int32)
    slots = jnp.arange(padded, dtype=jnp.int32)
    select = (rank[:, None, :] == slots[None, :, None]).astype(bf16)
    seg = col_width // 4
    lanes = jnp.arange(seg, dtype=jnp.int32)
    at_slot = rank[:, :, None] == lanes[None, None, :]
    slot_token = jnp.sum(jnp.where(at_slot, order[None, :, None], 0), axis=1).astype(f32)
    slot_weight = jnp.sum(jnp.where(at_slot, weight_hit[:, :, None], 0.0), axis=1)
    w_high = lax.reduce_precision(slot_weight, 8, 7)
    w_mid = lax.reduce_precision(slot_weight - w_high, 8, 7)
    w_low = slot_weight - w_high - w_mid
    notes = jnp.concatenate([slot_token, w_high, w_mid, w_low], axis=1)
    notes = jnp.where(slots[None, :, None] == capacity, notes[:, None, :], 0.0)

    share = tok_rows // tp_size
    places = [(tp_at ^ k) * col_width for k in range(tp_size)]
    partial_value = dot(gated_out, proj_out).astype(bf16)
    by_cols = jnp.stack(
        [lax.dynamic_slice_in_dim(partial_value, p, col_width, 1) for p in places], axis=0
    )
    pieces = []
    for k in range(tp_size):
        rows = lax.dynamic_slice_in_dim(by_cols, (tp_at ^ k) * share, share, 1)
        pieces.append(jnp.concatenate([by_cols[k]] + [rows[k ^ j] for j in range(tp_size)], axis=0))
    bit = 1
    while bit < tp_size:
        kept = [k for k in range(0, len(pieces)) if k % 2 == 0]
        given = jnp.stack([pieces[k + 1] for k in kept], axis=0)
        taken = swap(given, "tp", bit)
        pieces = [pieces[k].astype(f32) + taken[i].astype(f32) for i, k in enumerate(kept)]
        pieces = pieces[:1] + [p.astype(bf16) for p in pieces[1:]]
        bit *= 2
    mixer_sum = pieces[0]
    own_hidden = lax.dynamic_slice_in_dim(hidden, tp_at * col_width, col_width, 1)
    summed = (own_hidden.astype(f32) + mixer_sum[:tok_rows]).astype(bf16)

    sent = dot(select.reshape(experts_all * padded, tok_rows), summed)
    sent = (sent.reshape(experts_all, padded, col_width) + notes).astype(bf16)
    sent = sent.reshape(far, 2, local_experts, padded, col_width)
    passed = swap(sent[:, 1], "ep", 1)
    both_near = jnp.stack([sent[:, 0], passed], axis=1)
    grouped = [both_near[0]] + [swap(both_near[k], "ep", 2 * k) for k in range(1, far)]
    grouped = jnp.stack(grouped, axis=0)

    gain = ffn_gain.astype(f32)
    row_hidden = lax.dynamic_slice_in_dim(hidden, tp_at * share, share, 0)
    row_hidden = jnp.stack(
        [lax.dynamic_slice_in_dim(row_hidden, p, col_width, 1) for p in places], axis=0
    )
    row_gain = jnp.stack([lax.dynamic_slice_in_dim(gain, p, col_width, 0) for p in places], axis=0)
    rows = row_hidden.astype(f32) + mixer_sum[tok_rows:].reshape(tp_size, share, col_width)
    rows = rows.astype(bf16).astype(f32)
    squares = jnp.sum(jnp.sum(rows * rows, axis=2, keepdims=True), axis=0, keepdims=True)
    dense_in = (rows * lax.rsqrt(squares / width + epsilon) * row_gain[:, None]).astype(bf16)
    dense_near = jnp.stack(
        [dense_in] + [swap(dense_in, "ep", 2 * k) for k in range(1, far)], axis=0
    )
    dense_far = swap(dense_near, "ep", 1)
    dense_in = jnp.concatenate([dense_near, dense_far], axis=0)

    hidden_units = dense_gate.shape[1]
    total_share = ep_size * share
    both = jnp.zeros((total_share, 2 * hidden_units), f32)
    for k in range(tp_size):
        both = both + dot(dense_in[:, k].reshape(total_share, col_width), dense_rows[k])
    dense_act = (jax.nn.silu(both[:, :hidden_units]) * both[:, hidden_units:]).astype(bf16)
    act_pieces = spread_two_stage(dense_act, "tp")

    expert_rows = ep_size * capacity
    grouped = grouped.reshape(ep_size, local_experts, padded, col_width)
    note = grouped[:, :, capacity].astype(f32)
    expert_cols = grouped[:, :, :capacity].transpose(1, 0, 2, 3)
    expert_cols = expert_cols.reshape(local_experts * expert_rows, col_width)
    whole = jnp.zeros((local_experts * expert_rows, width), bf16)
    for k, piece in enumerate(spread_two_stage(expert_cols, "tp")):
        whole = lax.dynamic_update_slice_in_dim(whole, piece, places[k], 1)
    whole, dense_act = lax.optimization_barrier((whole, dense_act))
    floats = whole.astype(f32)
    expert_in = (floats * row_rsqrt(floats) * gain).astype(bf16)
    expert_in = expert_in.reshape(local_experts, expert_rows, width)
    gate_val = jnp.einsum("gid,gdf->gif", expert_in, expert_gate, preferred_element_type=f32)
    up_val = jnp.einsum("gid,gdf->gif", expert_in, expert_up, preferred_element_type=f32)
    inner_act = (jax.nn.silu(gate_val) * up_val).astype(bf16)
    partial_out = jnp.einsum("gif,gfd->gid", inner_act, expert_down, preferred_element_type=f32)
    partial_out = partial_out.astype(bf16).reshape(local_experts * expert_rows, width)
    pieces = [lax.dynamic_slice_in_dim(partial_out, p, col_width, 1) for p in places]
    bit = 1
    while bit < tp_size:
        kept = [k for k in range(0, len(pieces)) if k % 2 == 0]
        given = jnp.stack([pieces[k + 1] for k in kept], axis=0)
        taken = swap(given, "tp", bit)
        pieces = [pieces[k].astype(f32) + taken[i].astype(f32) for i, k in enumerate(kept)]
        pieces = pieces[:1] + [p.astype(bf16) for p in pieces[1:]]
        bit *= 2
    expert_row = pieces[0].astype(bf16)

    slot_of = note[:, :, :capacity]
    w_first = note[:, :, seg : seg + capacity]
    w_rest = note[:, :, 2 * seg : 2 * seg + capacity] + note[:, :, 3 * seg : 3 * seg + capacity]
    lines = jnp.arange(ep_size * tok_rows, dtype=jnp.int32)
    distance = jnp.arange(ep_size, dtype=jnp.int32)
    first_line = ((distance % 2) * far + distance // 2) * tok_rows

    def placing(values):
        values = values.transpose(1, 0, 2).reshape(1, -1)
        where_to = slot_of.transpose(1, 0, 2).astype(jnp.int32) + first_line[None, :, None]
        return jnp.where(where_to.reshape(1, -1) == lines[:, None], values, 0.0).astype(bf16)

    acts = jnp.zeros((ep_size, tp_size, share, hidden_units), bf16)
    for k, piece in enumerate(act_pieces):
        piece = piece.reshape(ep_size, 1, share, hidden_units)
        acts = lax.dynamic_update_slice_in_dim(acts, piece, tp_at ^ k, 1)

    branch = dot(acts.reshape(ep_size * tok_rows, hidden_units), dense_down)
    branch = branch * jax.nn.sigmoid(branch_gate)[None, :]
    branch = branch + dot(placing(w_first), expert_row) + dot(placing(w_rest), expert_row)
    branch = branch.astype(bf16).reshape(2, far, tok_rows, col_width)
    returned = branch[0].astype(f32) + swap(branch[1], "ep", 1).astype(f32)
    total = summed.astype(f32) + returned[0]
    for k in range(1, far):
        total = total + swap(returned[k].astype(bf16), "ep", 2 * k).astype(f32)
    return (total.astype(bf16), new_lru, window[:, 1:])


def solution(mesh):
    in_specs = (
        P("ep", None),
        P(),
        P("ep", "tp"),
        P("ep", "tp"),
        P(None, "tp"),
        P("tp", None, None),
        P("tp", None, None),
        P("tp"),
        P("tp", None),
        P("ep", None, "tp"),
        P("ep", "tp"),
        P(),
        P("ep", None),
        P("ep", None),
        P("ep", None, "tp"),
        P("ep", None, "tp"),
        P("ep", "tp", None),
        P("tp", "ep"),
        P("tp", "ep"),
        P("ep", "tp"),
        P("tp"),
    )
    out_specs = (P("ep", "tp"), P("ep", "tp"), P("ep", None, "tp"))
    return jax.shard_map(
        on_device, mesh=mesh, in_specs=in_specs, out_specs=out_specs, check_vma=False
    )
```

```python
import jax
import jax.numpy as jnp
from jax import lax
from jax.experimental import pallas as pl
from jax.experimental.pallas import tpu as pltpu
from jax.sharding import PartitionSpec as P

epsilon = 1e-06
decay_scale = 8.0
bf16 = jnp.bfloat16
f32 = jnp.float32


def swap(value, axis, bits):
    size = lax.axis_size(axis)
    return lax.ppermute(value, axis, [(i, i ^ bits) for i in range(size)])


def swap_all(values, axis, stride):
    return [values[0]] + [swap(v, axis, stride * k) for k, v in enumerate(values) if k]


def dot(a, b):
    return jnp.dot(a, b, preferred_element_type=f32)


def shape(*dims, dtype=bf16):
    return jax.ShapeDtypeStruct(dims, dtype)


def spread_over_tp(value):
    near = swap(value, "tp", 1)
    far = swap(value, "tp", 2)
    return [value, near, far, swap(far, "tp", 1)]


def local(body, outs, *args, scratch=(), at=None, pick=None, far_args=(), grant=16):
    specs = [
        pl.BlockSpec(memory_space=pltpu.HBM if i in far_args else pltpu.VMEM)
        for i in range(len(args))
    ]
    args = tuple(
        pltpu.with_memory_space_constraint(a, pltpu.HBM) if i in far_args else a
        for i, a in enumerate(args)
    )
    run = body
    if at is not None:
        args = (at,) + args
        specs = [pl.BlockSpec(memory_space=pltpu.SMEM)] + specs

        def run(number, *refs):
            body((pick(number[0]),), *refs)

    return pl.pallas_call(
        run,
        out_shape=outs,
        in_specs=specs,
        out_specs=jax.tree.map(lambda _: pl.BlockSpec(memory_space=pltpu.VMEM), outs),
        scratch_shapes=list(scratch),
        compiler_params=pltpu.CompilerParams(vmem_limit_bytes=grant << 20),
    )(*args)


def lanes_at(index, width):
    return pl.ds(pl.multiple_of(index * width, width), width)


def norm_body(far, at, hidden_far, gain, *rest):
    outs, (hidden, normed, sem) = rest[:-3], rest[-3:]
    copy = pltpu.make_async_copy(hidden_far, hidden, sem)
    copy.start()
    gains = gain[...].astype(f32)[None]
    copy.wait()
    floats = hidden[...].astype(f32)
    scale = lax.rsqrt(jnp.mean(floats * floats, axis=-1, keepdims=True) + epsilon)
    normed[...] = (floats * scale * gains).astype(bf16)
    width = hidden.shape[1] // far
    for k in range(far):
        outs[k][...] = normed[:, lanes_at(at[0] ^ k, width)]


def project_body(far, near, *refs):
    blocks, weights = refs[:far], refs[far : far + 4]
    outs, lhs = refs[far + 4 : far + 4 + far], refs[-1]
    rows = blocks[0].shape[0]
    for k in range(far):
        lhs[k * rows : (k + 1) * rows] = blocks[k][...]
    half = lhs.shape[1] // 2
    wide = weights[0].shape[1]
    for i in range(2):
        own, other = weights[2 * i][...], weights[2 * i + 1][...]
        upper = jnp.where(near[0] == 0, own, other)
        lower = jnp.where(near[0] == 0, other, own)
        part = dot(lhs[:, :half], upper) + dot(lhs[:, half:], lower)
        part = part.astype(bf16)
        for k in range(far):
            outs[k][:, i * wide : (i + 1) * wide] = part[k * rows : (k + 1) * rows]


def one_less_exp(value):
    series = 1.0 + value / 7.0 * (1.0 + value / 8.0)
    for n in (6.0, 5.0, 4.0, 3.0, 2.0):
        series = 1.0 + value / n * series
    return jnp.where(value > -0.35, -value * series, 1.0 - jnp.exp(value))


def mixer_body(far, tp_size, at, *refs):
    parts = refs[:far]
    window, taps, gates, decay, state, weights = refs[far : far + 6]
    new_state, new_window, keep, give, by_cols = refs[far + 6 :]
    wide = state.shape[1]
    total = parts[0][...].astype(f32)
    for k in range(1, far):
        total = total + parts[k][...].astype(f32)
    x_proj = total[:, :wide].astype(bf16)
    y_proj = total[:, wide:].astype(bf16)
    older = window.shape[0]
    conv = x_proj.astype(f32) * taps[older : older + 1].astype(f32)
    for i in range(older):
        conv = conv + window[i].astype(f32) * taps[i : i + 1].astype(f32)
        if i:
            new_window[i - 1] = window[i]
    new_window[older - 1] = x_proj
    conv = conv.astype(bf16)
    count, group = gates.shape[0], gates.shape[1]
    gate_in, gate_dec = [], []
    for g in range(count):
        both = dot(conv[:, g * group : (g + 1) * group], gates[g])
        gate_in.append(both[:, :group])
        gate_dec.append(both[:, group:])
    gate_in = jax.nn.sigmoid(jnp.concatenate(gate_in, axis=1))
    gate_dec = jax.nn.sigmoid(jnp.concatenate(gate_dec, axis=1))
    values = decay[...]
    log_sigmoid = jnp.minimum(values, 0.0) - jnp.log1p(jnp.exp(-jnp.abs(values)))
    log_decay = decay_scale * gate_dec * log_sigmoid
    inject = jnp.sqrt(one_less_exp(2.0 * log_decay))
    fresh = jnp.exp(log_decay) * state[...] + inject * gate_in * conv.astype(f32)
    new_state[...] = fresh
    gated = (fresh * jax.nn.gelu(y_proj.astype(f32))).astype(bf16)
    rows = gated.shape[0]
    share = rows // tp_size
    col_width = weights.shape[1] // tp_size
    for k in range(tp_size):
        part = dot(gated, weights[:, lanes_at(at[0] ^ k, col_width)]).astype(bf16)
        by_cols[k] = part
        (give if k % 2 else keep)[k // 2, :rows] = part
    for k in range(tp_size):
        to = give if k % 2 else keep
        for j in range(tp_size):
            first = rows + j * share
            to[k // 2, first : first + share] = by_cols[
                k ^ j, pl.ds(pl.multiple_of((at[0] ^ k) * share, share), share)
            ]


def prepare_body(far, capacity, at, *refs):
    *refs, sems = refs
    moved = (len(refs) - 3) // 2
    sources, (select, notes, gates), targets = refs[:moved], refs[moved : moved + 3], refs[moved + 3 :]
    copies = [
        pltpu.make_async_copy(source, target, sems.at[i])
        for i, (source, target) in enumerate(zip(sources, targets))
    ]
    for copy in copies:
        copy.start()
    for copy in copies[-4:]:
        copy.wait()
    routes, scores, in_gate, dec_gate = targets[-4:]
    count, tokens = 2 * far, routes.shape[1]
    padded = select.shape[0] // count
    seg = notes.shape[1] // 4
    place = lax.broadcasted_iota(jnp.int32, (count, 1), 0)
    near = (place >= far).astype(jnp.int32)
    ids = at[0] ^ (2 * (place - far * near) + near)
    hit = jnp.zeros((count, tokens), f32)
    score = jnp.zeros((count, tokens), f32)
    for i in range(routes.shape[0]):
        named = routes[i : i + 1] == ids
        hit = hit + jnp.where(named, 1.0, 0.0)
        score = score + jnp.where(named, scores[i : i + 1], 0.0)
    source = lax.broadcasted_iota(jnp.int32, (tokens, tokens), 0)
    target = lax.broadcasted_iota(jnp.int32, (tokens, tokens), 1)
    rank = dot(hit.astype(bf16), (source < target).astype(f32).astype(bf16))
    rank = jnp.where(hit > 0.0, rank, -1.0)
    high = score.astype(bf16)
    rest = score - high.astype(f32)
    mid = rest.astype(bf16)
    low = (rest - mid.astype(f32)).astype(bf16)
    order = lax.broadcasted_iota(jnp.int32, (1, tokens), 1).astype(f32).astype(bf16)
    slot = lax.broadcasted_iota(jnp.int32, (seg, tokens), 0).astype(f32)
    notes[...] = jnp.zeros(notes.shape, bf16)
    for i in range(count):
        taken = jnp.where(slot == rank[i : i + 1], 1.0, 0.0).astype(bf16)
        select[i * padded : (i + 1) * padded] = taken[:padded]
        line = i * padded + capacity
        for j, value in enumerate((order, high[i : i + 1], mid[i : i + 1], low[i : i + 1])):
            found = lax.dot_general(
                value, taken, (((1,), (1,)), ((), ())), preferred_element_type=f32
            )
            notes[line : line + 1, j * seg : (j + 1) * seg] = found.astype(bf16)
    size = in_gate.shape[1]
    pair = gates.shape[1] // size
    for g in range(gates.shape[0]):
        for h in range(pair):
            row = []
            for gate in (in_gate, dec_gate):
                for c in range(pair):
                    block = gate[g * pair + h]
                    row.append(block if c == h else jnp.zeros_like(block))
            gates[g, h * size : (h + 1) * size] = jnp.concatenate(row, axis=1)
    for copy in copies[:-4]:
        copy.wait()


def pass_on_body(kept, taken, out):
    out[...] = (kept[1].astype(f32) + taken[1].astype(f32)).astype(bf16)


def join_body(near, far, out):
    out[...] = (near[...].astype(f32) + far[...].astype(f32)).astype(bf16)


def final_body(count, summed, *refs):
    total = summed[...].astype(f32)
    for part in refs[:count]:
        total = total + part[...].astype(f32)
    refs[count][...] = total.astype(bf16)


def place_body(far, capacity, note, first, rest):
    count = note.shape[0]
    lines, slots = first.shape
    seg = note.shape[1] // 4
    tokens = lines // count
    column = lax.broadcasted_iota(jnp.int32, (count, slots), 1)
    owner = jnp.zeros((count, slots), jnp.int32)
    for k in range(1, count):
        owner = owner + (column >= k * capacity).astype(jnp.int32)
    here = owner == lax.broadcasted_iota(jnp.int32, (count, slots), 0)
    wide = jnp.zeros((seg, slots), jnp.int32)
    column = lax.broadcasted_iota(jnp.int32, (seg, slots), 1)
    for k in range(1, count):
        wide = wide + (column >= k * capacity).astype(jnp.int32)
    spread = lax.broadcasted_iota(jnp.int32, (seg, slots), 0) == column - wide * capacity
    spread = jnp.where(spread, 1.0, 0.0).astype(bf16)

    def across(part):
        values = dot(note[:, part * seg : (part + 1) * seg].astype(bf16), spread)
        return jnp.sum(jnp.where(here, values, 0.0), axis=0, keepdims=True)

    start = ((owner[:1] & 1) * far + (owner[:1] >> 1)) * tokens
    goal = across(0).astype(jnp.int32) + start
    there = lax.broadcasted_iota(jnp.int32, (lines, slots), 0) == goal
    first[...] = jnp.where(there, across(1), 0.0).astype(bf16)
    rest[...] = jnp.where(there, across(2) + across(3), 0.0).astype(bf16)


def route_body(tp_size, at, kept, taken, last, hidden, gain, select, notes, *outs):
    summed, stay, go, dense_in = outs
    mixer = kept[0].astype(f32) + taken[0].astype(f32) + last[...].astype(f32)
    rows, width = hidden.shape
    share = rows // tp_size
    col_width = width // tp_size
    own = hidden[:, lanes_at(at[0], col_width)].astype(f32)
    own = (own + mixer[:rows]).astype(bf16)
    summed[...] = own
    sent = (dot(select[...], own) + notes[...].astype(f32)).astype(bf16)
    stay[...] = sent[: stay.shape[0]]
    go[...] = sent[stay.shape[0] :]
    token_rows = pl.ds(pl.multiple_of(at[0] * share, share), share)
    whole, squares = [], 0.0
    for k in range(tp_size):
        first = rows + k * share
        part = hidden[token_rows, lanes_at(at[0] ^ k, col_width)].astype(f32)
        part = (part + mixer[first : first + share]).astype(bf16).astype(f32)
        whole.append(part)
        squares = squares + jnp.sum(part * part, axis=1, keepdims=True)
    scale = lax.rsqrt(squares / width + epsilon)
    for k in range(tp_size):
        gains = gain[:, lanes_at(at[0] ^ k, col_width)].astype(f32)
        dense_in[k * share : (k + 1) * share] = (whole[k] * scale * gains).astype(bf16)


def merge_body(far, stay, passed, *outs):
    rows = outs[0].shape[0] // 2
    for k in range(far):
        outs[k][:rows] = stay[k * rows : (k + 1) * rows]
        outs[k][rows:] = passed[k * rows : (k + 1) * rows]


def compact_body(far, padded, capacity, *refs):
    blocks, out, note, rows = refs[:far], refs[far], refs[far + 1], refs[far + 2]
    size = 2 * padded
    for k in range(far):
        rows[k * size : (k + 1) * size] = blocks[k][...]
        for i in range(2):
            line = i * padded + capacity
            note[2 * k + i : 2 * k + i + 1] = blocks[k][line : line + 1].astype(f32)
    count, total = out.shape[0], rows.shape[0]
    to = lax.broadcasted_iota(jnp.int32, (count, total), 0)
    source = lax.broadcasted_iota(jnp.int32, (count, total), 1)
    block = jnp.zeros((count, total), jnp.int32)
    for k in range(1, total // padded):
        block = block + (to >= k * capacity).astype(jnp.int32)
    pick = source == to + block * (padded - capacity)
    out[...] = dot(pick.astype(bf16), rows[...]).astype(bf16)


def expert_body(tp_size, at, *refs):
    pieces, gain, gate, up, down = refs[:tp_size], *refs[tp_size : tp_size + 4]
    keep, give = refs[tp_size + 4 :]
    width = pieces[0].shape[1]
    floats = [piece[...].astype(f32) for piece in pieces]
    squares = sum(jnp.sum(f * f, axis=1, keepdims=True) for f in floats)
    scale = lax.rsqrt(squares / gain.shape[1] + epsilon)
    gate_sum, up_sum = 0.0, 0.0
    for k in range(tp_size):
        gains = gain[:, lanes_at(at[0] ^ k, width)].astype(f32)
        rows = (floats[k] * scale * gains).astype(bf16)
        gate_sum = gate_sum + dot(rows, gate[lanes_at(at[0] ^ k, width)])
        up_sum = up_sum + dot(rows, up[lanes_at(at[0] ^ k, width)])
    act = (jax.nn.silu(gate_sum) * up_sum).astype(bf16)
    for k in range(tp_size):
        out = dot(act, down[:, lanes_at(at[0] ^ k, width)]).astype(bf16)
        (give if k % 2 else keep)[k // 2] = out


def dense_body(sources, tp_size, *refs):
    blocks = refs[:sources]
    gates, ups = refs[sources : sources + tp_size], refs[sources + tp_size : sources + 2 * tp_size]
    out, lhs = refs[sources + 2 * tp_size :]
    share = blocks[0].shape[0] // tp_size
    gate_sum, up_sum = 0.0, 0.0
    for k in range(tp_size):
        for m in range(sources):
            lhs[k, m * share : (m + 1) * share] = blocks[m][k * share : (k + 1) * share]
        gate_sum = gate_sum + dot(lhs[k], gates[k][...])
        up_sum = up_sum + dot(lhs[k], ups[k][...])
    out[...] = (jax.nn.silu(gate_sum) * up_sum).astype(bf16)


def down_body(tp_size, share, at, *refs):
    acts = refs[:tp_size]
    weights, gate, first, rest, kept, taken, last = refs[tp_size : tp_size + 7]
    outs, total = refs[tp_size + 7 : -1], refs[-1]
    rows = kept[0].astype(f32) + taken[0].astype(f32) + last[...].astype(f32)
    rows = rows.astype(bf16)
    total[...] = dot(first[...], rows) + dot(rest[...], rows)
    scale = jax.nn.sigmoid(gate[...])
    for k in range(tp_size):
        part = dot(acts[k][...], weights[...]) * scale
        for m in range(part.shape[0] // share):
            place = (m * tp_size + (at[0] ^ k)) * share
            spot = pl.ds(pl.multiple_of(place, share), share)
            total[spot] = total[spot] + part[m * share : (m + 1) * share]
    size = total.shape[0] // len(outs)
    for i, out in enumerate(outs):
        out[...] = total[i * size : (i + 1) * size].astype(bf16)


def on_device(
    hidden,
    mix_gain,
    proj_x,
    proj_y,
    conv_taps,
    input_gate,
    decay_gate,
    decay_param,
    proj_out,
    conv_state,
    lru_state,
    ffn_gain,
    routes,
    route_weights,
    expert_gate,
    expert_up,
    expert_down,
    dense_gate,
    dense_up,
    dense_down,
    branch_gate,
):
    tok_rows, width = hidden.shape
    ep_size = lax.axis_size("ep")
    tp_size = lax.axis_size("tp")
    at = (lax.axis_index("ep") * tp_size + lax.axis_index("tp")).astype(jnp.int32)[None]
    tp_bits = tp_size.bit_length() - 1

    def ep_at(number):
        return number >> tp_bits

    def far_at(number):
        return number >> (tp_bits + 1)

    def near(number):
        return (number >> tp_bits) & 1

    def tp_at(number):
        return number & (tp_size - 1)

    col_width = width // tp_size
    lru_local = lru_state.shape[1]
    far = ep_size // 2
    share = tok_rows // tp_size

    other_x = swap(proj_x, "ep", 1)
    other_y = swap(proj_y, "ep", 1)

    cols = local(
        lambda *refs: norm_body(far, *refs),
        [shape(tok_rows, width // far)] * far,
        hidden,
        mix_gain,
        far_args=(0,),
        scratch=[
            pltpu.VMEM((tok_rows, width), bf16),
            pltpu.VMEM((tok_rows, width), bf16),
            pltpu.SemaphoreType.DMA,
        ],
        at=at,
        pick=far_at,
    )
    spread = swap_all(cols, "ep", 2)

    gate_rows = spread_over_tp(dense_gate)
    up_rows = spread_over_tp(dense_up)

    top_count = routes.shape[1]
    experts_all = expert_gate.shape[0] * ep_size
    capacity = tok_rows * top_count // experts_all + 2
    padded = -(-(capacity + 1) // 8) * 8
    _, block_size = input_gate.shape[:2]
    group = max(block_size, 128)
    moved = [proj_x, proj_y, conv_state.transpose(1, 0, 2), lru_state, proj_out]
    small = [routes.T, route_weights.T, input_gate, decay_gate]
    select, notes, gates, *moved = local(
        lambda *refs: prepare_body(far, capacity, *refs),
        [
            shape(ep_size * padded, tok_rows),
            shape(ep_size * padded, col_width),
            shape(lru_local // group, group, 2 * group),
        ]
        + [shape(*m.shape, dtype=m.dtype) for m in moved],
        *moved,
        *small,
        far_args=range(len(moved) + len(small)),
        scratch=[pltpu.VMEM(m.shape, m.dtype) for m in small]
        + [pltpu.SemaphoreType.DMA((len(moved) + len(small),))],
        at=at,
        pick=ep_at,
    )

    parts = local(
        lambda *refs: project_body(far, *refs),
        [shape(tok_rows, 2 * lru_local)] * far,
        *spread,
        moved[0],
        other_x,
        moved[1],
        other_y,
        scratch=[pltpu.VMEM((far * tok_rows, width // far), bf16)],
        at=at,
        pick=near,
    )
    parts = swap_all(parts, "ep", 2)

    half = tp_size // 2
    new_lru, new_conv, keep, give = local(
        lambda *refs: mixer_body(far, tp_size, *refs),
        [
            shape(tok_rows, lru_local, dtype=f32),
            shape(conv_state.shape[1], tok_rows, lru_local),
            shape(half, 2 * tok_rows, col_width),
            shape(half, 2 * tok_rows, col_width),
        ],
        *parts,
        moved[2],
        conv_taps,
        gates,
        decay_param[None],
        moved[3],
        moved[4],
        scratch=[pltpu.VMEM((tp_size, tok_rows, col_width), bf16)],
        at=at,
        pick=tp_at,
    )
    new_conv = new_conv.transpose(1, 0, 2)
    taken = swap(give, "tp", 1)
    passed_on = local(pass_on_body, shape(2 * tok_rows, col_width), keep, taken)
    last = swap(passed_on, "tp", 2)

    summed, stay, go, dense_in = local(
        lambda *refs: route_body(tp_size, *refs),
        [
            shape(tok_rows, col_width),
            shape(far * padded, col_width),
            shape(far * padded, col_width),
            shape(tok_rows, col_width),
        ],
        keep,
        taken,
        last,
        hidden,
        ffn_gain[None],
        select,
        notes,
        at=at,
        pick=tp_at,
    )
    passed = swap(go, "ep", 1)
    dense_near = swap_all([dense_in] * far, "ep", 2)
    merged = local(
        lambda *refs: merge_body(far, *refs),
        [shape(2 * padded, col_width)] * far,
        stay,
        passed,
    )
    arrived = swap_all(merged, "ep", 2)
    dense_far = [swap(d, "ep", 1) for d in dense_near]

    expert_rows = ep_size * capacity
    expert_cols, note = local(
        lambda *refs: compact_body(far, padded, capacity, *refs),
        [shape(expert_rows, col_width), shape(ep_size, col_width, dtype=f32)],
        *arrived,
        scratch=[pltpu.VMEM((ep_size * padded, col_width), bf16)],
    )
    pieces = spread_over_tp(expert_cols)

    hidden_units = dense_gate.shape[1]
    dense_act = local(
        lambda *refs: dense_body(ep_size, tp_size, *refs),
        shape(ep_size * share, hidden_units),
        *dense_near,
        *dense_far,
        *gate_rows,
        *up_rows,
        scratch=[pltpu.VMEM((tp_size, ep_size * share, col_width), bf16)],
    )
    act_pieces = spread_over_tp(dense_act)

    expert_keep, expert_give = local(
        lambda *refs: expert_body(tp_size, *refs),
        [shape(half, expert_rows, col_width)] * 2,
        *pieces,
        ffn_gain[None],
        expert_gate[0],
        expert_up[0],
        expert_down[0],
        at=at,
        pick=tp_at,
    )
    expert_taken = swap(expert_give, "tp", 1)
    expert_on = local(
        pass_on_body, shape(expert_rows, col_width), expert_keep, expert_taken
    )
    expert_last = swap(expert_on, "tp", 2)
    first, rest = local(
        lambda *refs: place_body(far, capacity, *refs),
        [shape(ep_size * tok_rows, expert_rows)] * 2,
        note,
    )

    outs = local(
        lambda *refs: down_body(tp_size, share, *refs),
        [shape(tok_rows, col_width)] * ep_size,
        *act_pieces,
        dense_down,
        branch_gate[None],
        first,
        rest,
        expert_keep,
        expert_taken,
        expert_last,
        scratch=[pltpu.VMEM((ep_size * tok_rows, col_width), f32)],
        at=at,
        pick=tp_at,
    )
    returned = [swap(out, "ep", 1) for out in outs[far:]]
    joined = [
        local(join_body, shape(tok_rows, col_width), outs[k], returned[k])
        for k in range(1, far)
    ]
    arrived = [swap(j, "ep", 2 * k) for k, j in enumerate(joined, 1)]
    total = local(
        lambda *refs: final_body(ep_size // 2 + 1, *refs),
        shape(tok_rows, col_width),
        summed,
        outs[0],
        returned[0],
        *arrived,
    )
    return (total, new_lru, new_conv)


def solution(mesh):
    in_specs = (
        P("ep", None),
        P(),
        P("ep", "tp"),
        P("ep", "tp"),
        P(None, "tp"),
        P("tp", None, None),
        P("tp", None, None),
        P("tp"),
        P("tp", None),
        P("ep", None, "tp"),
        P("ep", "tp"),
        P(),
        P("ep", None),
        P("ep", None),
        P("ep", None, "tp"),
        P("ep", None, "tp"),
        P("ep", "tp", None),
        P("tp", "ep"),
        P("tp", "ep"),
        P("ep", "tp"),
        P("tp"),
    )
    out_specs = (P("ep", "tp"), P("ep", "tp"), P("ep", None, "tp"))
    return jax.shard_map(
        on_device, mesh=mesh, in_specs=in_specs, out_specs=out_specs, check_vma=False
    )
```

```python
import jax
import jax.numpy as jnp
from jax import lax
from jax.experimental import pallas as pl
from jax.experimental.pallas import tpu as pltpu
from jax.sharding import PartitionSpec as P

epsilon = 1e-06
decay_scale = 8.0
bf16 = jnp.bfloat16
f32 = jnp.float32


def swap(value, axis, bits):
    size = lax.axis_size(axis)
    return lax.ppermute(value, axis, [(i, i ^ bits) for i in range(size)])


def swap_all(values, axis, stride):
    return [values[0]] + [swap(v, axis, stride * k) for k, v in enumerate(values) if k]


def dot(a, b):
    return jnp.dot(a, b, preferred_element_type=f32)


def shape(*dims, dtype=bf16):
    return jax.ShapeDtypeStruct(dims, dtype)


def spread_over_tp(value):
    near = swap(value, "tp", 1)
    far = swap(value, "tp", 2)
    return [value, near, far, swap(far, "tp", 1)]


def local(body, outs, *args, scratch=(), at=None, pick=None, far_args=(), grant=16):
    specs = [
        pl.BlockSpec(memory_space=pltpu.HBM if i in far_args else pltpu.VMEM)
        for i in range(len(args))
    ]
    args = tuple(
        pltpu.with_memory_space_constraint(a, pltpu.HBM) if i in far_args else a
        for i, a in enumerate(args)
    )
    run = body
    if at is not None:
        args = (at,) + args
        specs = [pl.BlockSpec(memory_space=pltpu.SMEM)] + specs

        def run(number, *refs):
            body((pick(number[0]),), *refs)

    return pl.pallas_call(
        run,
        out_shape=outs,
        in_specs=specs,
        out_specs=jax.tree.map(lambda _: pl.BlockSpec(memory_space=pltpu.VMEM), outs),
        scratch_shapes=list(scratch),
        compiler_params=pltpu.CompilerParams(vmem_limit_bytes=grant << 20),
    )(*args)


def lanes_at(index, width):
    return pl.ds(pl.multiple_of(index * width, width), width)


def norm_body(far, at, hidden_far, gain, *rest):
    outs, (hidden, gains, normed, sems) = rest[:-4], rest[-4:]
    copies = [
        pltpu.make_async_copy(hidden_far, hidden, sems.at[0]),
        pltpu.make_async_copy(gain, gains, sems.at[1]),
    ]
    for copy in copies:
        copy.start()
    for copy in copies:
        copy.wait()
    floats = hidden[...].astype(f32)
    scale = lax.rsqrt(jnp.mean(floats * floats, axis=-1, keepdims=True) + epsilon)
    normed[...] = (floats * scale * gains[...].astype(f32)[None]).astype(bf16)
    width = hidden.shape[1] // far
    for k in range(far):
        outs[k][...] = normed[:, lanes_at(at[0] ^ k, width)]


def project_body(far, near, *refs):
    blocks, weights = refs[:far], refs[far : far + 4]
    outs, lhs = refs[far + 4 : far + 4 + far], refs[-1]
    rows = blocks[0].shape[0]
    for k in range(far):
        lhs[k * rows : (k + 1) * rows] = blocks[k][...]
    half = lhs.shape[1] // 2
    wide = weights[0].shape[1]
    for i in range(2):
        own, other = weights[2 * i][...], weights[2 * i + 1][...]
        upper = jnp.where(near[0] == 0, own, other)
        lower = jnp.where(near[0] == 0, other, own)
        part = dot(lhs[:, :half], upper) + dot(lhs[:, half:], lower)
        part = part.astype(bf16)
        for k in range(far):
            outs[k][:, i * wide : (i + 1) * wide] = part[k * rows : (k + 1) * rows]


def one_less_exp(value):
    series = 1.0 + value / 7.0 * (1.0 + value / 8.0)
    for n in (6.0, 5.0, 4.0, 3.0, 2.0):
        series = 1.0 + value / n * series
    return jnp.where(value > -0.35, -value * series, 1.0 - jnp.exp(value))


def mixer_body(far, tp_size, at, *refs):
    parts = refs[:far]
    window, taps, gates, decay, state, weights = refs[far : far + 6]
    new_state, new_window, keep, give, by_cols = refs[far + 6 :]
    wide = state.shape[1]
    total = parts[0][...].astype(f32)
    for k in range(1, far):
        total = total + parts[k][...].astype(f32)
    x_proj = total[:, :wide].astype(bf16)
    y_proj = total[:, wide:].astype(bf16)
    older = window.shape[0]
    conv = x_proj.astype(f32) * taps[older : older + 1].astype(f32)
    for i in range(older):
        conv = conv + window[i].astype(f32) * taps[i : i + 1].astype(f32)
        if i:
            new_window[i - 1] = window[i]
    new_window[older - 1] = x_proj
    conv = conv.astype(bf16)
    count, group = gates.shape[0], gates.shape[1]
    gate_in, gate_dec = [], []
    for g in range(count):
        both = dot(conv[:, g * group : (g + 1) * group], gates[g])
        gate_in.append(both[:, :group])
        gate_dec.append(both[:, group:])
    gate_in = jax.nn.sigmoid(jnp.concatenate(gate_in, axis=1))
    gate_dec = jax.nn.sigmoid(jnp.concatenate(gate_dec, axis=1))
    values = decay[...]
    log_sigmoid = jnp.minimum(values, 0.0) - jnp.log1p(jnp.exp(-jnp.abs(values)))
    log_decay = decay_scale * gate_dec * log_sigmoid
    inject = jnp.sqrt(one_less_exp(2.0 * log_decay))
    fresh = jnp.exp(log_decay) * state[...] + inject * gate_in * conv.astype(f32)
    new_state[...] = fresh
    gated = (fresh * jax.nn.gelu(y_proj.astype(f32))).astype(bf16)
    rows = gated.shape[0]
    share = rows // tp_size
    col_width = weights.shape[1] // tp_size
    for k in range(tp_size):
        part = dot(gated, weights[:, lanes_at(at[0] ^ k, col_width)]).astype(bf16)
        by_cols[k] = part
        (give if k % 2 else keep)[k // 2, :rows] = part
    for k in range(tp_size):
        to = give if k % 2 else keep
        for j in range(tp_size):
            first = rows + j * share
            to[k // 2, first : first + share] = by_cols[
                k ^ j, pl.ds(pl.multiple_of((at[0] ^ k) * share, share), share)
            ]


def prepare_body(far, capacity, at, *refs):
    *refs, sems = refs
    moved = (len(refs) - 3) // 2
    sources, (select, notes, gates), targets = refs[:moved], refs[moved : moved + 3], refs[moved + 3 :]
    copies = [
        pltpu.make_async_copy(source, target, sems.at[i])
        for i, (source, target) in enumerate(zip(sources, targets))
    ]
    for copy in copies:
        copy.start()
    for copy in copies[-4:]:
        copy.wait()
    routes, scores, in_gate, dec_gate = targets[-4:]
    count, tokens = 2 * far, routes.shape[1]
    padded = select.shape[0] // count
    seg = notes.shape[1] // 4
    place = lax.broadcasted_iota(jnp.int32, (count, 1), 0)
    near = (place >= far).astype(jnp.int32)
    ids = at[0] ^ (2 * (place - far * near) + near)
    hit = jnp.zeros((count, tokens), f32)
    score = jnp.zeros((count, tokens), f32)
    for i in range(routes.shape[0]):
        named = routes[i : i + 1] == ids
        hit = hit + jnp.where(named, 1.0, 0.0)
        score = score + jnp.where(named, scores[i : i + 1], 0.0)
    source = lax.broadcasted_iota(jnp.int32, (tokens, tokens), 0)
    target = lax.broadcasted_iota(jnp.int32, (tokens, tokens), 1)
    rank = dot(hit.astype(bf16), (source < target).astype(f32).astype(bf16))
    rank = jnp.where(hit > 0.0, rank, -1.0)
    high = score.astype(bf16)
    rest = score - high.astype(f32)
    mid = rest.astype(bf16)
    low = (rest - mid.astype(f32)).astype(bf16)
    order = lax.broadcasted_iota(jnp.int32, (1, tokens), 1).astype(f32).astype(bf16)
    slot = lax.broadcasted_iota(jnp.int32, (seg, tokens), 0).astype(f32)
    notes[...] = jnp.zeros(notes.shape, bf16)
    for i in range(count):
        taken = jnp.where(slot == rank[i : i + 1], 1.0, 0.0).astype(bf16)
        select[i * padded : (i + 1) * padded] = taken[:padded]
        line = i * padded + capacity
        for j, value in enumerate((order, high[i : i + 1], mid[i : i + 1], low[i : i + 1])):
            found = lax.dot_general(
                value, taken, (((1,), (1,)), ((), ())), preferred_element_type=f32
            )
            notes[line : line + 1, j * seg : (j + 1) * seg] = found.astype(bf16)
    size = in_gate.shape[1]
    pair = gates.shape[1] // size
    for g in range(gates.shape[0]):
        for h in range(pair):
            row = []
            for gate in (in_gate, dec_gate):
                for c in range(pair):
                    block = gate[g * pair + h]
                    row.append(block if c == h else jnp.zeros_like(block))
            gates[g, h * size : (h + 1) * size] = jnp.concatenate(row, axis=1)
    for copy in copies[:-4]:
        copy.wait()


def pass_on_body(kept, taken, out):
    out[...] = (kept[1].astype(f32) + taken[1].astype(f32)).astype(bf16)


def join_body(near, far, out):
    out[...] = (near[...].astype(f32) + far[...].astype(f32)).astype(bf16)


def final_body(count, summed, *refs):
    total = summed[...].astype(f32)
    for part in refs[:count]:
        total = total + part[...].astype(f32)
    refs[count][...] = total.astype(bf16)


def place_body(far, capacity, note, first, rest):
    count = note.shape[0]
    lines, slots = first.shape
    seg = note.shape[1] // 4
    tokens = lines // count
    column = lax.broadcasted_iota(jnp.int32, (count, slots), 1)
    owner = jnp.zeros((count, slots), jnp.int32)
    for k in range(1, count):
        owner = owner + (column >= k * capacity).astype(jnp.int32)
    here = owner == lax.broadcasted_iota(jnp.int32, (count, slots), 0)
    wide = jnp.zeros((seg, slots), jnp.int32)
    column = lax.broadcasted_iota(jnp.int32, (seg, slots), 1)
    for k in range(1, count):
        wide = wide + (column >= k * capacity).astype(jnp.int32)
    spread = lax.broadcasted_iota(jnp.int32, (seg, slots), 0) == column - wide * capacity
    spread = jnp.where(spread, 1.0, 0.0).astype(bf16)

    def across(part):
        values = dot(note[:, part * seg : (part + 1) * seg].astype(bf16), spread)
        return jnp.sum(jnp.where(here, values, 0.0), axis=0, keepdims=True)

    start = ((owner[:1] & 1) * far + (owner[:1] >> 1)) * tokens
    goal = across(0).astype(jnp.int32) + start
    there = lax.broadcasted_iota(jnp.int32, (lines, slots), 0) == goal
    first[...] = jnp.where(there, across(1), 0.0).astype(bf16)
    rest[...] = jnp.where(there, across(2) + across(3), 0.0).astype(bf16)


def route_body(tp_size, at, kept, taken, last, hidden, gain, select, notes, *outs):
    summed, stay, go, dense_in = outs
    mixer = kept[0].astype(f32) + taken[0].astype(f32) + last[...].astype(f32)
    rows, width = hidden.shape
    share = rows // tp_size
    col_width = width // tp_size
    own = hidden[:, lanes_at(at[0], col_width)].astype(f32)
    own = (own + mixer[:rows]).astype(bf16)
    summed[...] = own
    sent = (dot(select[...], own) + notes[...].astype(f32)).astype(bf16)
    stay[...] = sent[: stay.shape[0]]
    go[...] = sent[stay.shape[0] :]
    token_rows = pl.ds(pl.multiple_of(at[0] * share, share), share)
    whole, squares = [], 0.0
    for k in range(tp_size):
        first = rows + k * share
        part = hidden[token_rows, lanes_at(at[0] ^ k, col_width)].astype(f32)
        part = (part + mixer[first : first + share]).astype(bf16).astype(f32)
        whole.append(part)
        squares = squares + jnp.sum(part * part, axis=1, keepdims=True)
    scale = lax.rsqrt(squares / width + epsilon)
    for k in range(tp_size):
        gains = gain[:, lanes_at(at[0] ^ k, col_width)].astype(f32)
        dense_in[k * share : (k + 1) * share] = (whole[k] * scale * gains).astype(bf16)


def merge_body(far, stay, passed, *outs):
    rows = outs[0].shape[0] // 2
    for k in range(far):
        outs[k][:rows] = stay[k * rows : (k + 1) * rows]
        outs[k][rows:] = passed[k * rows : (k + 1) * rows]


def compact_body(far, padded, capacity, *refs):
    blocks, out, note, rows = refs[:far], refs[far], refs[far + 1], refs[far + 2]
    size = 2 * padded
    for k in range(far):
        rows[k * size : (k + 1) * size] = blocks[k][...]
        for i in range(2):
            line = i * padded + capacity
            note[2 * k + i : 2 * k + i + 1] = blocks[k][line : line + 1].astype(f32)
    count, total = out.shape[0], rows.shape[0]
    to = lax.broadcasted_iota(jnp.int32, (count, total), 0)
    source = lax.broadcasted_iota(jnp.int32, (count, total), 1)
    block = jnp.zeros((count, total), jnp.int32)
    for k in range(1, total // padded):
        block = block + (to >= k * capacity).astype(jnp.int32)
    pick = source == to + block * (padded - capacity)
    out[...] = dot(pick.astype(bf16), rows[...]).astype(bf16)


def expert_body(tp_size, at, *refs):
    pieces, gain, gate, up, down = refs[:tp_size], *refs[tp_size : tp_size + 4]
    keep, give = refs[tp_size + 4 :]
    width = pieces[0].shape[1]
    floats = [piece[...].astype(f32) for piece in pieces]
    squares = sum(jnp.sum(f * f, axis=1, keepdims=True) for f in floats)
    scale = lax.rsqrt(squares / gain.shape[1] + epsilon)
    gate_sum, up_sum = 0.0, 0.0
    for k in range(tp_size):
        gains = gain[:, lanes_at(at[0] ^ k, width)].astype(f32)
        rows = (floats[k] * scale * gains).astype(bf16)
        gate_sum = gate_sum + dot(rows, gate[lanes_at(at[0] ^ k, width)])
        up_sum = up_sum + dot(rows, up[lanes_at(at[0] ^ k, width)])
    act = (jax.nn.silu(gate_sum) * up_sum).astype(bf16)
    for k in range(tp_size):
        out = dot(act, down[:, lanes_at(at[0] ^ k, width)]).astype(bf16)
        (give if k % 2 else keep)[k // 2] = out


def dense_body(sources, tp_size, *refs):
    blocks = refs[:sources]
    gates, ups = refs[sources : sources + tp_size], refs[sources + tp_size : sources + 2 * tp_size]
    out, lhs = refs[sources + 2 * tp_size :]
    share = blocks[0].shape[0] // tp_size
    gate_sum, up_sum = 0.0, 0.0
    for k in range(tp_size):
        for m in range(sources):
            lhs[k, m * share : (m + 1) * share] = blocks[m][k * share : (k + 1) * share]
        gate_sum = gate_sum + dot(lhs[k], gates[k][...])
        up_sum = up_sum + dot(lhs[k], ups[k][...])
    out[...] = (jax.nn.silu(gate_sum) * up_sum).astype(bf16)


def down_body(tp_size, share, at, *refs):
    acts = refs[:tp_size]
    weights, gate, first, rest, kept, taken, last = refs[tp_size : tp_size + 7]
    outs, total = refs[tp_size + 7 : -1], refs[-1]
    rows = kept[0].astype(f32) + taken[0].astype(f32) + last[...].astype(f32)
    rows = rows.astype(bf16)
    total[...] = dot(first[...], rows) + dot(rest[...], rows)
    scale = jax.nn.sigmoid(gate[...])
    for k in range(tp_size):
        part = dot(acts[k][...], weights[...]) * scale
        for m in range(part.shape[0] // share):
            place = (m * tp_size + (at[0] ^ k)) * share
            spot = pl.ds(pl.multiple_of(place, share), share)
            total[spot] = total[spot] + part[m * share : (m + 1) * share]
    size = total.shape[0] // len(outs)
    for i, out in enumerate(outs):
        out[...] = total[i * size : (i + 1) * size].astype(bf16)


def on_device(
    hidden,
    mix_gain,
    proj_x,
    proj_y,
    conv_taps,
    input_gate,
    decay_gate,
    decay_param,
    proj_out,
    conv_state,
    lru_state,
    ffn_gain,
    routes,
    route_weights,
    expert_gate,
    expert_up,
    expert_down,
    dense_gate,
    dense_up,
    dense_down,
    branch_gate,
):
    tok_rows, width = hidden.shape
    ep_size = lax.axis_size("ep")
    tp_size = lax.axis_size("tp")
    at = (lax.axis_index("ep") * tp_size + lax.axis_index("tp")).astype(jnp.int32)[None]
    tp_bits = tp_size.bit_length() - 1

    def ep_at(number):
        return number >> tp_bits

    def far_at(number):
        return number >> (tp_bits + 1)

    def near(number):
        return (number >> tp_bits) & 1

    def tp_at(number):
        return number & (tp_size - 1)

    col_width = width // tp_size
    lru_local = lru_state.shape[1]
    far = ep_size // 2
    share = tok_rows // tp_size

    other_x = swap(proj_x, "ep", 1)
    other_y = swap(proj_y, "ep", 1)

    cols = local(
        lambda *refs: norm_body(far, *refs),
        [shape(tok_rows, width // far)] * far,
        hidden,
        mix_gain,
        far_args=(0, 1),
        scratch=[
            pltpu.VMEM((tok_rows, width), bf16),
            pltpu.VMEM((width,), bf16),
            pltpu.VMEM((tok_rows, width), bf16),
            pltpu.SemaphoreType.DMA((2,)),
        ],
        at=at,
        pick=far_at,
    )
    spread = swap_all(cols, "ep", 2)

    gate_rows = spread_over_tp(dense_gate)
    up_rows = spread_over_tp(dense_up)

    top_count = routes.shape[1]
    experts_all = expert_gate.shape[0] * ep_size
    capacity = tok_rows * top_count // experts_all + 2
    padded = -(-(capacity + 1) // 8) * 8
    _, block_size = input_gate.shape[:2]
    group = max(block_size, 128)
    moved = [proj_x, proj_y, conv_state.transpose(1, 0, 2), lru_state, proj_out]
    small = [routes.T, route_weights.T, input_gate, decay_gate]
    select, notes, gates, *moved = local(
        lambda *refs: prepare_body(far, capacity, *refs),
        [
            shape(ep_size * padded, tok_rows),
            shape(ep_size * padded, col_width),
            shape(lru_local // group, group, 2 * group),
        ]
        + [shape(*m.shape, dtype=m.dtype) for m in moved],
        *moved,
        *small,
        far_args=range(len(moved) + len(small)),
        scratch=[pltpu.VMEM(m.shape, m.dtype) for m in small]
        + [pltpu.SemaphoreType.DMA((len(moved) + len(small),))],
        at=at,
        pick=ep_at,
    )

    parts = local(
        lambda *refs: project_body(far, *refs),
        [shape(tok_rows, 2 * lru_local)] * far,
        *spread,
        moved[0],
        other_x,
        moved[1],
        other_y,
        scratch=[pltpu.VMEM((far * tok_rows, width // far), bf16)],
        at=at,
        pick=near,
    )
    parts = swap_all(parts, "ep", 2)

    half = tp_size // 2
    new_lru, new_conv, keep, give = local(
        lambda *refs: mixer_body(far, tp_size, *refs),
        [
            shape(tok_rows, lru_local, dtype=f32),
            shape(conv_state.shape[1], tok_rows, lru_local),
            shape(half, 2 * tok_rows, col_width),
            shape(half, 2 * tok_rows, col_width),
        ],
        *parts,
        moved[2],
        conv_taps,
        gates,
        decay_param[None],
        moved[3],
        moved[4],
        scratch=[pltpu.VMEM((tp_size, tok_rows, col_width), bf16)],
        at=at,
        pick=tp_at,
    )
    new_conv = new_conv.transpose(1, 0, 2)
    taken = swap(give, "tp", 1)
    passed_on = local(pass_on_body, shape(2 * tok_rows, col_width), keep, taken)
    last = swap(passed_on, "tp", 2)

    summed, stay, go, dense_in = local(
        lambda *refs: route_body(tp_size, *refs),
        [
            shape(tok_rows, col_width),
            shape(far * padded, col_width),
            shape(far * padded, col_width),
            shape(tok_rows, col_width),
        ],
        keep,
        taken,
        last,
        hidden,
        ffn_gain[None],
        select,
        notes,
        at=at,
        pick=tp_at,
    )
    passed = swap(go, "ep", 1)
    dense_near = swap_all([dense_in] * far, "ep", 2)
    merged = local(
        lambda *refs: merge_body(far, *refs),
        [shape(2 * padded, col_width)] * far,
        stay,
        passed,
    )
    arrived = swap_all(merged, "ep", 2)
    dense_far = [swap(d, "ep", 1) for d in dense_near]

    expert_rows = ep_size * capacity
    expert_cols, note = local(
        lambda *refs: compact_body(far, padded, capacity, *refs),
        [shape(expert_rows, col_width), shape(ep_size, col_width, dtype=f32)],
        *arrived,
        scratch=[pltpu.VMEM((ep_size * padded, col_width), bf16)],
    )
    pieces = spread_over_tp(expert_cols)

    hidden_units = dense_gate.shape[1]
    dense_act = local(
        lambda *refs: dense_body(ep_size, tp_size, *refs),
        shape(ep_size * share, hidden_units),
        *dense_near,
        *dense_far,
        *gate_rows,
        *up_rows,
        scratch=[pltpu.VMEM((tp_size, ep_size * share, col_width), bf16)],
    )
    act_pieces = spread_over_tp(dense_act)

    expert_keep, expert_give = local(
        lambda *refs: expert_body(tp_size, *refs),
        [shape(half, expert_rows, col_width)] * 2,
        *pieces,
        ffn_gain[None],
        expert_gate[0],
        expert_up[0],
        expert_down[0],
        at=at,
        pick=tp_at,
    )
    expert_taken = swap(expert_give, "tp", 1)
    expert_on = local(
        pass_on_body, shape(expert_rows, col_width), expert_keep, expert_taken
    )
    expert_last = swap(expert_on, "tp", 2)
    first, rest = local(
        lambda *refs: place_body(far, capacity, *refs),
        [shape(ep_size * tok_rows, expert_rows)] * 2,
        note,
    )

    outs = local(
        lambda *refs: down_body(tp_size, share, *refs),
        [shape(tok_rows, col_width)] * ep_size,
        *act_pieces,
        dense_down,
        branch_gate[None],
        first,
        rest,
        expert_keep,
        expert_taken,
        expert_last,
        scratch=[pltpu.VMEM((ep_size * tok_rows, col_width), f32)],
        at=at,
        pick=tp_at,
    )
    returned = [swap(out, "ep", 1) for out in outs[far:]]
    joined = [
        local(join_body, shape(tok_rows, col_width), outs[k], returned[k])
        for k in range(1, far)
    ]
    arrived = [swap(j, "ep", 2 * k) for k, j in enumerate(joined, 1)]
    total = local(
        lambda *refs: final_body(ep_size // 2 + 1, *refs),
        shape(tok_rows, col_width),
        summed,
        outs[0],
        returned[0],
        *arrived,
    )
    return (total, new_lru, new_conv)


def solution(mesh):
    in_specs = (
        P("ep", None),
        P(),
        P("ep", "tp"),
        P("ep", "tp"),
        P(None, "tp"),
        P("tp", None, None),
        P("tp", None, None),
        P("tp"),
        P("tp", None),
        P("ep", None, "tp"),
        P("ep", "tp"),
        P(),
        P("ep", None),
        P("ep", None),
        P("ep", None, "tp"),
        P("ep", None, "tp"),
        P("ep", "tp", None),
        P("tp", "ep"),
        P("tp", "ep"),
        P("ep", "tp"),
        P("tp"),
    )
    out_specs = (P("ep", "tp"), P("ep", "tp"), P("ep", None, "tp"))
    return jax.shard_map(
        on_device, mesh=mesh, in_specs=in_specs, out_specs=out_specs, check_vma=False
    )
```

```python
import jax
import jax.numpy as jnp
from jax import lax
from jax.experimental import pallas as pl
from jax.experimental.pallas import tpu as pltpu
from jax.sharding import PartitionSpec as P

epsilon = 1e-06
decay_scale = 8.0
bf16 = jnp.bfloat16
f32 = jnp.float32


def swap(value, axis, bits):
    size = lax.axis_size(axis)
    return lax.ppermute(value, axis, [(i, i ^ bits) for i in range(size)])


def swap_all(values, axis, stride):
    return [values[0]] + [swap(v, axis, stride * k) for k, v in enumerate(values) if k]


def dot(a, b):
    return jnp.dot(a, b, preferred_element_type=f32)


def shape(*dims, dtype=bf16):
    return jax.ShapeDtypeStruct(dims, dtype)


def spread_over_tp(value):
    near = swap(value, "tp", 1)
    far = swap(value, "tp", 2)
    return [value, near, far, swap(far, "tp", 1)]


def local(body, outs, *args, scratch=(), at=None, pick=None, far_args=(), grant=16):
    specs = [
        pl.BlockSpec(memory_space=pltpu.HBM if i in far_args else pltpu.VMEM)
        for i in range(len(args))
    ]
    args = tuple(
        pltpu.with_memory_space_constraint(a, pltpu.HBM) if i in far_args else a
        for i, a in enumerate(args)
    )
    run = body
    if at is not None:
        args = (at,) + args
        specs = [pl.BlockSpec(memory_space=pltpu.SMEM)] + specs

        def run(number, *refs):
            body((pick(number[0]),), *refs)

    return pl.pallas_call(
        run,
        out_shape=outs,
        in_specs=specs,
        out_specs=jax.tree.map(lambda _: pl.BlockSpec(memory_space=pltpu.VMEM), outs),
        scratch_shapes=list(scratch),
        compiler_params=pltpu.CompilerParams(vmem_limit_bytes=grant << 20),
    )(*args)


def lanes_at(index, width):
    return pl.ds(pl.multiple_of(index * width, width), width)


def norm_body(far, at, hidden_far, gain, *rest):
    outs, (hidden, gains, normed, sems) = rest[:-4], rest[-4:]
    copies = [
        pltpu.make_async_copy(hidden_far, hidden, sems.at[0]),
        pltpu.make_async_copy(gain, gains, sems.at[1]),
    ]
    for copy in copies:
        copy.start()
    for copy in copies:
        copy.wait()
    floats = hidden[...].astype(f32)
    scale = lax.rsqrt(jnp.mean(floats * floats, axis=-1, keepdims=True) + epsilon)
    normed[...] = (floats * scale * gains[...].astype(f32)[None]).astype(bf16)
    width = hidden.shape[1] // far
    for k in range(far):
        outs[k][...] = normed[:, lanes_at(at[0] ^ k, width)]


def project_body(far, near, *refs):
    blocks, weights = refs[:far], refs[far : far + 4]
    outs, lhs = refs[far + 4 : far + 4 + far], refs[-1]
    rows = blocks[0].shape[0]
    for k in range(far):
        lhs[k * rows : (k + 1) * rows] = blocks[k][...]
    half = lhs.shape[1] // 2
    wide = weights[0].shape[1]
    for i in range(2):
        own, other = weights[2 * i][...], weights[2 * i + 1][...]
        upper = jnp.where(near[0] == 0, own, other)
        lower = jnp.where(near[0] == 0, other, own)
        part = dot(lhs[:, :half], upper) + dot(lhs[:, half:], lower)
        part = part.astype(bf16)
        for k in range(far):
            outs[k][:, i * wide : (i + 1) * wide] = part[k * rows : (k + 1) * rows]


def one_less_exp(value):
    series = 1.0 + value / 7.0 * (1.0 + value / 8.0)
    for n in (6.0, 5.0, 4.0, 3.0, 2.0):
        series = 1.0 + value / n * series
    return jnp.where(value > -0.35, -value * series, 1.0 - jnp.exp(value))


def mixer_body(far, tp_size, at, *refs):
    parts = refs[:far]
    window, taps, gates, decay, state, weights = refs[far : far + 6]
    new_state, new_window, keep, give, by_cols = refs[far + 6 :]
    wide = state.shape[1]
    total = parts[0][...].astype(f32)
    for k in range(1, far):
        total = total + parts[k][...].astype(f32)
    x_proj = total[:, :wide].astype(bf16)
    y_proj = total[:, wide:].astype(bf16)
    older = window.shape[0]
    conv = x_proj.astype(f32) * taps[older : older + 1].astype(f32)
    for i in range(older):
        conv = conv + window[i].astype(f32) * taps[i : i + 1].astype(f32)
        if i:
            new_window[i - 1] = window[i]
    new_window[older - 1] = x_proj
    conv = conv.astype(bf16)
    count, group = gates.shape[0], gates.shape[1]
    gate_in, gate_dec = [], []
    for g in range(count):
        both = dot(conv[:, g * group : (g + 1) * group], gates[g])
        gate_in.append(both[:, :group])
        gate_dec.append(both[:, group:])
    gate_in = jax.nn.sigmoid(jnp.concatenate(gate_in, axis=1))
    gate_dec = jax.nn.sigmoid(jnp.concatenate(gate_dec, axis=1))
    values = decay[...]
    log_sigmoid = jnp.minimum(values, 0.0) - jnp.log1p(jnp.exp(-jnp.abs(values)))
    log_decay = decay_scale * gate_dec * log_sigmoid
    inject = jnp.sqrt(one_less_exp(2.0 * log_decay))
    fresh = jnp.exp(log_decay) * state[...] + inject * gate_in * conv.astype(f32)
    new_state[...] = fresh
    gated = (fresh * jax.nn.gelu(y_proj.astype(f32))).astype(bf16)
    rows = gated.shape[0]
    share = rows // tp_size
    col_width = weights.shape[1] // tp_size
    for k in range(tp_size):
        part = dot(gated, weights[:, lanes_at(at[0] ^ k, col_width)]).astype(bf16)
        by_cols[k] = part
        (give if k % 2 else keep)[k // 2, :rows] = part
    for k in range(tp_size):
        to = give if k % 2 else keep
        for j in range(tp_size):
            first = rows + j * share
            to[k // 2, first : first + share] = by_cols[
                k ^ j, pl.ds(pl.multiple_of((at[0] ^ k) * share, share), share)
            ]


def prepare_body(far, capacity, at, *refs):
    *refs, sems = refs
    moved = (len(refs) - 6) // 2
    sources, split, (select, notes, gates) = refs[:moved], refs[moved], refs[moved + 1 : moved + 4]
    halves, targets = refs[moved + 4 : moved + 6], refs[moved + 6 :]
    pairs = [(split.at[: halves[0].shape[0]], halves[0])]
    pairs += [(split.at[halves[0].shape[0] :], halves[1])]
    pairs += list(zip(sources, targets))
    copies = [
        pltpu.make_async_copy(source, target, sems.at[i])
        for i, (source, target) in enumerate(pairs)
    ]
    for copy in copies:
        copy.start()
    for copy in copies[-4:]:
        copy.wait()
    routes, scores, in_gate, dec_gate = targets[-4:]
    count, tokens = 2 * far, routes.shape[1]
    padded = select.shape[0] // count
    seg = notes.shape[1] // 4
    place = lax.broadcasted_iota(jnp.int32, (count, 1), 0)
    near = (place >= far).astype(jnp.int32)
    ids = at[0] ^ (2 * (place - far * near) + near)
    hit = jnp.zeros((count, tokens), f32)
    score = jnp.zeros((count, tokens), f32)
    for i in range(routes.shape[0]):
        named = routes[i : i + 1] == ids
        hit = hit + jnp.where(named, 1.0, 0.0)
        score = score + jnp.where(named, scores[i : i + 1], 0.0)
    source = lax.broadcasted_iota(jnp.int32, (tokens, tokens), 0)
    target = lax.broadcasted_iota(jnp.int32, (tokens, tokens), 1)
    rank = dot(hit.astype(bf16), (source < target).astype(f32).astype(bf16))
    rank = jnp.where(hit > 0.0, rank, -1.0)
    high = score.astype(bf16)
    rest = score - high.astype(f32)
    mid = rest.astype(bf16)
    low = (rest - mid.astype(f32)).astype(bf16)
    order = lax.broadcasted_iota(jnp.int32, (1, tokens), 1).astype(f32).astype(bf16)
    slot = lax.broadcasted_iota(jnp.int32, (seg, tokens), 0).astype(f32)
    notes[...] = jnp.zeros(notes.shape, bf16)
    for i in range(count):
        taken = jnp.where(slot == rank[i : i + 1], 1.0, 0.0).astype(bf16)
        select[i * padded : (i + 1) * padded] = taken[:padded]
        line = i * padded + capacity
        for j, value in enumerate((order, high[i : i + 1], mid[i : i + 1], low[i : i + 1])):
            found = lax.dot_general(
                value, taken, (((1,), (1,)), ((), ())), preferred_element_type=f32
            )
            notes[line : line + 1, j * seg : (j + 1) * seg] = found.astype(bf16)
    size = in_gate.shape[1]
    pair = gates.shape[1] // size
    for g in range(gates.shape[0]):
        for h in range(pair):
            row = []
            for gate in (in_gate, dec_gate):
                for c in range(pair):
                    block = gate[g * pair + h]
                    row.append(block if c == h else jnp.zeros_like(block))
            gates[g, h * size : (h + 1) * size] = jnp.concatenate(row, axis=1)
    for copy in copies[:-4]:
        copy.wait()


def pass_on_body(kept, taken, out):
    out[...] = (kept[1].astype(f32) + taken[1].astype(f32)).astype(bf16)


def join_body(near, far, out):
    out[...] = (near[...].astype(f32) + far[...].astype(f32)).astype(bf16)


def final_body(count, summed, *refs):
    total = summed[...].astype(f32)
    for part in refs[:count]:
        total = total + part[...].astype(f32)
    refs[count][...] = total.astype(bf16)


def place_body(far, capacity, note, first, rest):
    count = note.shape[0]
    lines, slots = first.shape
    seg = note.shape[1] // 4
    tokens = lines // count
    column = lax.broadcasted_iota(jnp.int32, (count, slots), 1)
    owner = jnp.zeros((count, slots), jnp.int32)
    for k in range(1, count):
        owner = owner + (column >= k * capacity).astype(jnp.int32)
    here = owner == lax.broadcasted_iota(jnp.int32, (count, slots), 0)
    wide = jnp.zeros((seg, slots), jnp.int32)
    column = lax.broadcasted_iota(jnp.int32, (seg, slots), 1)
    for k in range(1, count):
        wide = wide + (column >= k * capacity).astype(jnp.int32)
    spread = lax.broadcasted_iota(jnp.int32, (seg, slots), 0) == column - wide * capacity
    spread = jnp.where(spread, 1.0, 0.0).astype(bf16)

    def across(part):
        values = dot(note[:, part * seg : (part + 1) * seg].astype(bf16), spread)
        return jnp.sum(jnp.where(here, values, 0.0), axis=0, keepdims=True)

    start = ((owner[:1] & 1) * far + (owner[:1] >> 1)) * tokens
    goal = across(0).astype(jnp.int32) + start
    there = lax.broadcasted_iota(jnp.int32, (lines, slots), 0) == goal
    first[...] = jnp.where(there, across(1), 0.0).astype(bf16)
    rest[...] = jnp.where(there, across(2) + across(3), 0.0).astype(bf16)


def route_body(tp_size, at, kept, taken, last, hidden, gain, select, notes, *outs):
    summed, stay, go, dense_in = outs
    mixer = kept[0].astype(f32) + taken[0].astype(f32) + last[...].astype(f32)
    rows, width = hidden.shape
    share = rows // tp_size
    col_width = width // tp_size
    own = hidden[:, lanes_at(at[0], col_width)].astype(f32)
    own = (own + mixer[:rows]).astype(bf16)
    summed[...] = own
    sent = (dot(select[...], own) + notes[...].astype(f32)).astype(bf16)
    stay[...] = sent[: stay.shape[0]]
    go[...] = sent[stay.shape[0] :]
    token_rows = pl.ds(pl.multiple_of(at[0] * share, share), share)
    whole, squares = [], 0.0
    for k in range(tp_size):
        first = rows + k * share
        part = hidden[token_rows, lanes_at(at[0] ^ k, col_width)].astype(f32)
        part = (part + mixer[first : first + share]).astype(bf16).astype(f32)
        whole.append(part)
        squares = squares + jnp.sum(part * part, axis=1, keepdims=True)
    scale = lax.rsqrt(squares / width + epsilon)
    for k in range(tp_size):
        gains = gain[:, lanes_at(at[0] ^ k, col_width)].astype(f32)
        dense_in[k * share : (k + 1) * share] = (whole[k] * scale * gains).astype(bf16)


def merge_body(far, stay, passed, *outs):
    rows = outs[0].shape[0] // 2
    for k in range(far):
        outs[k][:rows] = stay[k * rows : (k + 1) * rows]
        outs[k][rows:] = passed[k * rows : (k + 1) * rows]


def compact_body(far, padded, capacity, *refs):
    blocks, out, note, rows = refs[:far], refs[far], refs[far + 1], refs[far + 2]
    size = 2 * padded
    for k in range(far):
        rows[k * size : (k + 1) * size] = blocks[k][...]
        for i in range(2):
            line = i * padded + capacity
            note[2 * k + i : 2 * k + i + 1] = blocks[k][line : line + 1].astype(f32)
    count, total = out.shape[0], rows.shape[0]
    to = lax.broadcasted_iota(jnp.int32, (count, total), 0)
    source = lax.broadcasted_iota(jnp.int32, (count, total), 1)
    block = jnp.zeros((count, total), jnp.int32)
    for k in range(1, total // padded):
        block = block + (to >= k * capacity).astype(jnp.int32)
    pick = source == to + block * (padded - capacity)
    out[...] = dot(pick.astype(bf16), rows[...]).astype(bf16)


def expert_body(tp_size, at, *refs):
    pieces, gain, gate, up, down = refs[:tp_size], *refs[tp_size : tp_size + 4]
    keep, give = refs[tp_size + 4 :]
    width = pieces[0].shape[1]
    floats = [piece[...].astype(f32) for piece in pieces]
    squares = sum(jnp.sum(f * f, axis=1, keepdims=True) for f in floats)
    scale = lax.rsqrt(squares / gain.shape[1] + epsilon)
    gate_sum, up_sum = 0.0, 0.0
    for k in range(tp_size):
        gains = gain[:, lanes_at(at[0] ^ k, width)].astype(f32)
        rows = (floats[k] * scale * gains).astype(bf16)
        gate_sum = gate_sum + dot(rows, gate[lanes_at(at[0] ^ k, width)])
        up_sum = up_sum + dot(rows, up[lanes_at(at[0] ^ k, width)])
    act = (jax.nn.silu(gate_sum) * up_sum).astype(bf16)
    for k in range(tp_size):
        out = dot(act, down[:, lanes_at(at[0] ^ k, width)]).astype(bf16)
        (give if k % 2 else keep)[k // 2] = out


def dense_body(sources, tp_size, *refs):
    blocks, gates = refs[:sources], refs[sources : sources + tp_size]
    ups, (out, lhs) = refs[sources + tp_size : -2], refs[-2:]
    share = blocks[0].shape[0] // tp_size
    gate_sum, up_sum = 0.0, 0.0
    for k in range(tp_size):
        for m in range(sources):
            lhs[k, m * share : (m + 1) * share] = blocks[m][k * share : (k + 1) * share]
        gate_sum = gate_sum + dot(lhs[k], gates[k][...])
        if k < 2:
            up_sum = up_sum + dot(lhs[k], ups[k][...])
        else:
            low, high = ups[2 * k - 2], ups[2 * k - 1]
            cut = low.shape[0]
            up_sum = up_sum + dot(lhs[k, :, :cut], low[...]) + dot(lhs[k, :, cut:], high[...])
    out[...] = (jax.nn.silu(gate_sum) * up_sum).astype(bf16)


def down_body(tp_size, share, at, *refs):
    acts = refs[:tp_size]
    weights, gate, total = refs[tp_size:]
    scale = jax.nn.sigmoid(gate[...])
    for k in range(tp_size):
        part = dot(acts[k][...], weights[...]) * scale
        for m in range(part.shape[0] // share):
            place = (m * tp_size + (at[0] ^ k)) * share
            spot = pl.ds(pl.multiple_of(place, share), share)
            total[spot] = part[m * share : (m + 1) * share]


def both_body(total, first, rest, kept, taken, last, *outs):
    rows = kept[0].astype(f32) + taken[0].astype(f32) + last[...].astype(f32)
    rows = rows.astype(bf16)
    size = outs[0].shape[0]
    for i, out in enumerate(outs):
        lines = slice(i * size, (i + 1) * size)
        part = dot(first[lines], rows) + dot(rest[lines], rows)
        out[...] = (total[lines] + part).astype(bf16)


def on_device(
    hidden,
    mix_gain,
    proj_x,
    proj_y,
    conv_taps,
    input_gate,
    decay_gate,
    decay_param,
    proj_out,
    conv_state,
    lru_state,
    ffn_gain,
    routes,
    route_weights,
    expert_gate,
    expert_up,
    expert_down,
    dense_gate,
    dense_up,
    dense_down,
    branch_gate,
):
    tok_rows, width = hidden.shape
    ep_size = lax.axis_size("ep")
    tp_size = lax.axis_size("tp")
    at = (lax.axis_index("ep") * tp_size + lax.axis_index("tp")).astype(jnp.int32)[None]
    tp_bits = tp_size.bit_length() - 1

    def ep_at(number):
        return number >> tp_bits

    def far_at(number):
        return number >> (tp_bits + 1)

    def near(number):
        return (number >> tp_bits) & 1

    def tp_at(number):
        return number & (tp_size - 1)

    col_width = width // tp_size
    lru_local = lru_state.shape[1]
    far = ep_size // 2
    share = tok_rows // tp_size

    other_x = swap(proj_x, "ep", 1)
    other_y = swap(proj_y, "ep", 1)

    cols = local(
        lambda *refs: norm_body(far, *refs),
        [shape(tok_rows, width // far)] * far,
        hidden,
        mix_gain,
        far_args=(0, 1),
        scratch=[
            pltpu.VMEM((tok_rows, width), bf16),
            pltpu.VMEM((width,), bf16),
            pltpu.VMEM((tok_rows, width), bf16),
            pltpu.SemaphoreType.DMA((2,)),
        ],
        at=at,
        pick=far_at,
    )
    spread = swap_all(cols, "ep", 2)

    gate_rows = spread_over_tp(dense_gate)
    up_near = swap(dense_up, "tp", 1)

    top_count = routes.shape[1]
    experts_all = expert_gate.shape[0] * ep_size
    capacity = tok_rows * top_count // experts_all + 2
    padded = -(-(capacity + 1) // 8) * 8
    _, block_size = input_gate.shape[:2]
    group = max(block_size, 128)
    moved = [proj_x, proj_y, conv_state.transpose(1, 0, 2), lru_state, proj_out]
    small = [routes.T, route_weights.T, input_gate, decay_gate]
    up_half = shape(dense_up.shape[0] // 2, dense_up.shape[1])
    select, notes, gates, up_low, up_high, *moved = local(
        lambda *refs: prepare_body(far, capacity, *refs),
        [
            shape(ep_size * padded, tok_rows),
            shape(ep_size * padded, col_width),
            shape(lru_local // group, group, 2 * group),
            up_half,
            up_half,
        ]
        + [shape(*m.shape, dtype=m.dtype) for m in moved],
        *moved,
        *small,
        dense_up,
        far_args=range(len(moved) + len(small) + 1),
        scratch=[pltpu.VMEM(m.shape, m.dtype) for m in small]
        + [pltpu.SemaphoreType.DMA((len(moved) + len(small) + 2,))],
        at=at,
        pick=ep_at,
    )

    far_ups = [swap(up_low, "tp", 2), swap(up_high, "tp", 2)]
    on_ups = [swap(far_ups[0], "tp", 1), swap(far_ups[1], "tp", 1)]

    parts = local(
        lambda *refs: project_body(far, *refs),
        [shape(tok_rows, 2 * lru_local)] * far,
        *spread,
        moved[0],
        other_x,
        moved[1],
        other_y,
        scratch=[pltpu.VMEM((far * tok_rows, width // far), bf16)],
        at=at,
        pick=near,
    )
    parts = swap_all(parts, "ep", 2)

    half = tp_size // 2
    new_lru, new_conv, keep, give = local(
        lambda *refs: mixer_body(far, tp_size, *refs),
        [
            shape(tok_rows, lru_local, dtype=f32),
            shape(conv_state.shape[1], tok_rows, lru_local),
            shape(half, 2 * tok_rows, col_width),
            shape(half, 2 * tok_rows, col_width),
        ],
        *parts,
        moved[2],
        conv_taps,
        gates,
        decay_param[None],
        moved[3],
        moved[4],
        scratch=[pltpu.VMEM((tp_size, tok_rows, col_width), bf16)],
        at=at,
        pick=tp_at,
    )
    new_conv = new_conv.transpose(1, 0, 2)
    taken = swap(give, "tp", 1)
    passed_on = local(pass_on_body, shape(2 * tok_rows, col_width), keep, taken)
    last = swap(passed_on, "tp", 2)

    summed, stay, go, dense_in = local(
        lambda *refs: route_body(tp_size, *refs),
        [
            shape(tok_rows, col_width),
            shape(far * padded, col_width),
            shape(far * padded, col_width),
            shape(tok_rows, col_width),
        ],
        keep,
        taken,
        last,
        hidden,
        ffn_gain[None],
        select,
        notes,
        at=at,
        pick=tp_at,
    )
    passed = swap(go, "ep", 1)
    dense_near = swap_all([dense_in] * far, "ep", 2)
    merged = local(
        lambda *refs: merge_body(far, *refs), [shape(2 * padded, col_width)] * far, stay, passed
    )
    arrived = swap_all(merged, "ep", 2)
    dense_far = [swap(d, "ep", 1) for d in dense_near]

    expert_rows = ep_size * capacity
    expert_cols, note = local(
        lambda *refs: compact_body(far, padded, capacity, *refs),
        [shape(expert_rows, col_width), shape(ep_size, col_width, dtype=f32)],
        *arrived,
        scratch=[pltpu.VMEM((ep_size * padded, col_width), bf16)],
    )
    pieces = spread_over_tp(expert_cols)

    hidden_units = dense_gate.shape[1]
    dense_act = local(
        lambda *refs: dense_body(ep_size, tp_size, *refs),
        shape(ep_size * share, hidden_units),
        *dense_near,
        *dense_far,
        *gate_rows,
        dense_up,
        up_near,
        *far_ups,
        *on_ups,
        scratch=[pltpu.VMEM((tp_size, ep_size * share, col_width), bf16)],
    )
    act_pieces = spread_over_tp(dense_act)

    expert_keep, expert_give = local(
        lambda *refs: expert_body(tp_size, *refs),
        [shape(half, expert_rows, col_width)] * 2,
        *pieces,
        ffn_gain[None],
        expert_gate[0],
        expert_up[0],
        expert_down[0],
        at=at,
        pick=tp_at,
    )
    expert_taken = swap(expert_give, "tp", 1)
    expert_on = local(pass_on_body, shape(expert_rows, col_width), expert_keep, expert_taken)
    expert_last = swap(expert_on, "tp", 2)
    first, rest = local(
        lambda *refs: place_body(far, capacity, *refs),
        [shape(ep_size * tok_rows, expert_rows)] * 2,
        note,
    )

    dense_out = local(
        lambda *refs: down_body(tp_size, share, *refs),
        shape(ep_size * tok_rows, col_width, dtype=f32),
        *act_pieces,
        dense_down,
        branch_gate[None],
        at=at,
        pick=tp_at,
    )
    outs = local(
        both_body,
        [shape(tok_rows, col_width)] * ep_size,
        dense_out,
        first,
        rest,
        expert_keep,
        expert_taken,
        expert_last,
    )
    returned = [swap(out, "ep", 1) for out in outs[far:]]
    joined = [
        local(join_body, shape(tok_rows, col_width), outs[k], returned[k])
        for k in range(1, far)
    ]
    arrived = [swap(j, "ep", 2 * k) for k, j in enumerate(joined, 1)]
    total = local(
        lambda *refs: final_body(ep_size // 2 + 1, *refs),
        shape(tok_rows, col_width),
        summed,
        outs[0],
        returned[0],
        *arrived,
    )
    return (total, new_lru, new_conv)


def solution(mesh):
    in_specs = (
        P("ep", None),
        P(),
        P("ep", "tp"),
        P("ep", "tp"),
        P(None, "tp"),
        P("tp", None, None),
        P("tp", None, None),
        P("tp"),
        P("tp", None),
        P("ep", None, "tp"),
        P("ep", "tp"),
        P(),
        P("ep", None),
        P("ep", None),
        P("ep", None, "tp"),
        P("ep", None, "tp"),
        P("ep", "tp", None),
        P("tp", "ep"),
        P("tp", "ep"),
        P("ep", "tp"),
        P("tp"),
    )
    out_specs = (P("ep", "tp"), P("ep", "tp"), P("ep", None, "tp"))
    return jax.shard_map(
        on_device, mesh=mesh, in_specs=in_specs, out_specs=out_specs, check_vma=False
    )
```
